256 devices in a mesh: grp: 2 (over y), fs: 32 (over z, core), tp: 4 (over x).
Axes of the slice: x: 4, y: 2, z: 16, core: 2. Of those that a mesh axis runs over, the one named last changes fastest.
The devices are a block of a 4x16x16 slice.
Arguments:
- tokens: bfloat16 [4096, 2048], P(('grp', 'fs')), parts along dimension 0, may hold values from -6 to 6
- routes: int32 [4096, 2], P(('grp', 'fs')), parts along dimension 0, may hold values from 0 to 3, as said below
- route_logits: float32 [4096, 2], P(('grp', 'fs')), parts along dimension 0, may hold values from -8 to 8
- gain: float32 [2048], P('fs'), may hold values from 0.1 to 1.9
- w_gate: float32 [4, 2048, 7168], P(None, 'fs', 'tp'), may hold values from -0.125 to 0.125
- w_up: float32 [4, 2048, 7168], P(None, 'fs', 'tp'), may hold values from -0.125 to 0.125
- w_down: float32 [4, 7168, 2048], P(None, 'fs', 'tp'), may hold values from -0.0625 to 0.0625
Outputs:
- gate_served: bfloat16 [8, 2048, 7168], P(('grp', 'tp'), None, 'fs'), parts along dimension 0
- up_served: bfloat16 [8, 2048, 7168], P(('grp', 'tp'), None, 'fs'), parts along dimension 0
- down_served: bfloat16 [8, 7168, 2048], P(('grp', 'tp'), 'fs'), parts along dimension 0
- mixed: bfloat16 [4096, 2048], P(('grp', 'fs'), 'tp'), parts along dimension 0
The draws below stay inside these ranges and needn't reach their ends.
There are 2 independent parts, one for each index of `grp`. The reference program is written for one: setup_inputs(seed, part) draws one part's arguments, and reference() takes and returns one part's arrays. A program takes and returns all parts, laid end to end along the dimension named above; an argument that names none is the same for every part. Nothing has to cross between parts.
Inputs may be any that keep to these rules, and one draw needn't show every extreme that they name: `routes`: each row names 2 different experts; every expert is named by some row.
All inputs are finite; a program needn't handle non-finite values.
Results may differ from the reference program's by a relative error of at most 0.0085.
Values may be sent and summed in bfloat16 or wider, within the bound.
No kernel may reach another device: no remote copies, remote signals or barrier semaphores. Data moves between devices by JAX's collectives and lax.ppermute only.
A program may use at most 128 MiB of HBM per device.

```python
import jax
import jax.numpy as jnp
from jax import lax

D = 2048
FF = 7168
EXPERTS = 4
TOP = 2
TOKENS = 2048


def draw_routes(key, part):
    key_hot = jax.random.fold_in(key, 101)
    key_pick = jax.random.fold_in(key, 102)
    key_other = jax.random.fold_in(key, 103)
    key_second = jax.random.fold_in(key, 104)
    hot_expert = jax.random.randint(key_hot, (), 0, EXPERTS, dtype=jnp.int32)
    chooser = jax.random.randint(key_pick, (TOKENS,), 0, 8, dtype=jnp.int32)
    other_offset = jax.random.randint(key_other, (TOKENS,), 0, EXPERTS - 1, dtype=jnp.int32)
    other_expert = (hot_expert + 1 + other_offset) % EXPERTS
    first_col = jnp.where(chooser < 7, hot_expert, other_expert).astype(jnp.int32)
    second_offset = jax.random.randint(key_second, (TOKENS,), 0, EXPERTS - 1, dtype=jnp.int32)
    second_col = ((first_col + 1 + second_offset) % EXPERTS).astype(jnp.int32)
    row_index = jnp.arange(TOKENS, dtype=jnp.int32)
    first_col = jnp.where(row_index < EXPERTS, row_index, first_col)
    second_col = jnp.where(row_index < EXPERTS, (row_index + 1) % EXPERTS, second_col)
    return jnp.stack([first_col, second_col], axis=1).astype(jnp.int32)


def steps_of(stream_key, extent, pieces, low, largest):
    def one(axis_at, shards_of):
        draws = jax.random.uniform(jax.random.fold_in(jax.random.fold_in(stream_key, 6), axis_at), (shards_of,), jnp.float32, low / len(pieces), largest / len(pieces))
        return jnp.repeat(jnp.exp(draws), extent[axis_at] // shards_of).reshape((-1,) + (1,) * (len(extent) - axis_at - 1))

    level = one(*pieces[0])
    for cut in pieces[1:]:
        level = level * one(*cut)
    return level


def gaussian(stream_key, dims, width, reach, split=(), held_as=jnp.bfloat16):
    array = jax.random.normal(stream_key, dims, jnp.float32) * width
    if len(split) > 0:
        array = steps_of(stream_key, dims, split, -0.22, 0.18) * array
    return jnp.clip(array, min=-reach, max=reach).astype(held_as)


def setup_inputs(seed: int = 0, part: int = 0) -> dict:
    splits = jax.random.split(jax.random.key(seed), 8)
    own_keys = jax.random.split(jax.random.fold_in(splits[7], part), 8)
    tokens = gaussian(own_keys[0], (TOKENS, D), 1.0, 6.0, ((0, 32),))
    routes = draw_routes(jax.random.fold_in(jax.random.fold_in(splits[7], part), 71), part)
    route_logits = gaussian(own_keys[2], (TOKENS, TOP), 1.5, 8.0, ((0, 32),), jnp.float32)
    gain = jnp.clip(1.0 + 0.18 * jax.random.normal(splits[3], (D,), jnp.float32), 0.1, 1.9)
    w_gate = gaussian(splits[4], (EXPERTS, D, FF), D ** -0.5, 0.125, ((1, 32), (2, 4)), jnp.float32)
    w_up = gaussian(splits[5], (EXPERTS, D, FF), D ** -0.5, 0.125, ((1, 32), (2, 4)), jnp.float32)
    w_down = gaussian(splits[6], (EXPERTS, FF, D), FF ** -0.5, 0.0625, ((1, 32), (2, 4)), jnp.float32)
    return {"tokens": tokens, "routes": routes, "route_logits": route_logits, "gain": gain, "w_gate": w_gate, "w_up": w_up, "w_down": w_down}


def reference(tokens, routes, route_logits, gain, w_gate, w_up, w_down):
    values = tokens.astype(jnp.float32)
    mean_square = lax.optimization_barrier(jnp.mean(values * values, axis=-1, keepdims=True))
    normed = (values * lax.rsqrt(mean_square + 1e-06)).astype(jnp.bfloat16)
    first = jax.nn.sigmoid(route_logits[:, 0] - route_logits[:, 1])
    second = jax.nn.sigmoid(route_logits[:, 1] - route_logits[:, 0])
    gate_cast = (w_gate * gain[None, :, None]).astype(jnp.bfloat16)
    up_cast = (w_up * gain[None, :, None]).astype(jnp.bfloat16)
    down_cast = w_down.astype(jnp.bfloat16)
    total = jnp.zeros((tokens.shape[0], w_down.shape[2]), jnp.float32)
    for expert in range(EXPERTS):
        weight_col = first * (routes[:, 0] == expert).astype(jnp.float32)
        weight_col = weight_col + second * (routes[:, 1] == expert).astype(jnp.float32)
        weight_col = weight_col.astype(jnp.bfloat16)
        gate_act = jnp.dot(normed, gate_cast[expert], preferred_element_type=jnp.float32)
        up_act = jnp.dot(normed, up_cast[expert], preferred_element_type=jnp.float32)
        hidden = (jax.nn.silu(gate_act) * up_act * weight_col[:, None].astype(jnp.float32)).astype(jnp.bfloat16)
        total = total + jnp.dot(hidden, down_cast[expert], preferred_element_type=jnp.float32)
    return (gate_cast, up_cast, down_cast, total.astype(jnp.bfloat16))
```

```python
import functools

import jax
import jax.numpy as jnp
from jax import lax
from jax.experimental import pallas as pl
from jax.experimental.pallas import tpu as pltpu
from jax.sharding import PartitionSpec as P

BF16, F32 = jnp.bfloat16, jnp.float32
LANES = 128
VMEM = 56 * 1024 * 1024


def params(*semantics):
    return pltpu.CompilerParams(dimension_semantics=semantics, vmem_limit_bytes=VMEM)


def pack_kernel(parts, width, scale_ref, gate_ref, up_ref, *out_refs):
    both = jnp.concatenate([gate_ref[0], up_ref[0]], axis=0)
    columns = (both.T * scale_ref[...]).astype(BF16)
    for k in range(columns.shape[0] // width):
        for out_ref, (low, size) in zip(out_refs, parts):
            at = k * width + low
            out_ref[0, k] = columns[at : at + size]


def pack(gain, w_gate, w_up, parts, width):
    experts, rows, columns = w_gate.shape
    scale = jnp.concatenate([gain, gain])[None, :]
    blocks = columns // width
    return pl.pallas_call(
        functools.partial(pack_kernel, parts, width),
        grid=(experts,),
        in_specs=[
            pl.BlockSpec((1, 2 * rows), lambda e: (0, 0)),
            pl.BlockSpec((1, rows, columns), lambda e: (e, 0, 0)),
            pl.BlockSpec((1, rows, columns), lambda e: (e, 0, 0)),
        ],
        out_specs=[
            pl.BlockSpec((1, blocks, size, 2 * rows), lambda e: (e, 0, 0, 0)) for _, size in parts
        ],
        out_shape=[
            jax.ShapeDtypeStruct((experts, blocks, size, 2 * rows), BF16) for _, size in parts
        ],
        compiler_params=params("arbitrary"),
        cost_estimate=pl.CostEstimate(
            flops=experts * rows * columns * 200, bytes_accessed=experts * rows * columns * 12, transcendentals=0
        ),
        name="pack",
    )(scale, w_gate, w_up)


def unpack_kernel(size, recv_ref, gate_ref, up_ref, both_ref):
    half = recv_ref.shape[2] // 2
    pad = both_ref.shape[0] // 2 - size
    if pad:
        zeros = jnp.zeros((pad, both_ref.shape[1]), BF16)
        both_ref[size : size + pad] = zeros
        both_ref[size + pad + size :] = zeros
    for k in range(recv_ref.shape[0] // 2):
        one, two = recv_ref[2 * k], recv_ref[2 * k + 1]
        at = slice(k * 2 * half, (k + 1) * 2 * half)
        gate = jnp.concatenate([one[:, :half], two[:, :half]], axis=1)
        up = jnp.concatenate([one[:, half:], two[:, half:]], axis=1)
        gate_ref[:, at] = gate
        up_ref[:, at] = up
        both_ref[0:size, at] = gate
        both_ref[size + pad : size + pad + size, at] = up


def unpack(recv, padded):
    count, size, lanes = recv.shape
    width = count * lanes // 2
    return pl.pallas_call(
        functools.partial(unpack_kernel, size),
        in_specs=[pl.BlockSpec(memory_space=pltpu.VMEM)],
        out_specs=[pl.BlockSpec(memory_space=pltpu.VMEM)] * 3,
        out_shape=[
            jax.ShapeDtypeStruct((size, width), BF16),
            jax.ShapeDtypeStruct((size, width), BF16),
            jax.ShapeDtypeStruct((2 * padded, width), BF16),
        ],
        compiler_params=params(),
        cost_estimate=pl.CostEstimate(flops=count * size * lanes * 40, bytes_accessed=count * size * lanes * 6, transcendentals=0),
        name="unpack",
    )(recv)


def hidden_kernel(depth, expert_ref, tokens_ref, both_ref, out_ref):
    owners, rows = tokens_ref.shape[0], tokens_ref.shape[2]
    block = tokens_ref[...].reshape(owners * rows, tokens_ref.shape[3])
    acts = lax.dot_general(
        block[:, :depth], both_ref[...], (((1,), (1,)), ((), ())), preferred_element_type=F32
    )
    shares = block[:, depth:].astype(F32)
    lane = lax.broadcasted_iota(jnp.int32, shares.shape, 1)
    share = jnp.sum(jnp.where(lane == expert_ref[0], shares, 0.0), axis=1, keepdims=True)
    half = acts.shape[1] // 2
    gate, up = acts[:, :half], acts[:, half:]
    hidden = gate / (1.0 + jnp.exp(-gate)) * up * share
    out_ref[...] = hidden.astype(BF16).reshape(1, owners, rows, half)


def hidden_of(expert, tokens, both, depth, first, count, owners):
    n_owner, _, rows, wide = tokens.shape
    half = both.shape[0] // 2
    work = count * n_owner * rows
    return pl.pallas_call(
        functools.partial(hidden_kernel, depth),
        grid=(count, n_owner // owners),
        in_specs=[
            pl.BlockSpec(memory_space=pltpu.SMEM),
            pl.BlockSpec((owners, 1, rows, wide), lambda q, i: (i, q + first, 0, 0)),
            pl.BlockSpec(both.shape, lambda q, i: (0, 0)),
        ],
        out_specs=pl.BlockSpec((1, owners, rows, half), lambda q, i: (q, i, 0, 0)),
        out_shape=jax.ShapeDtypeStruct((count, n_owner, rows, half), BF16),
        compiler_params=params("arbitrary", "arbitrary"),
        cost_estimate=pl.CostEstimate(
            flops=2 * work * depth * 2 * half, bytes_accessed=work * wide * 2 + both.size * 2, transcendentals=work * half
        ),
        name="hidden",
    )(expert, tokens, both)


def down_kernel(experts, place_ref, down_ref, *refs):
    parts, (keep_ref, send_ref) = refs[:-2], refs[-2:]
    per = len(parts) // experts
    total = None
    for shift in range(experts):
        pieces = []
        for p in range(per):
            r = parts[p * experts + shift]
            pieces.append(r[...].reshape(-1, r.shape[-1]))
        source = lax.rem(place_ref[0] + experts - shift, experts)
        left = jnp.concatenate(pieces, axis=1) if per > 1 else pieces[0]
        term = jnp.dot(left, down_ref[source], preferred_element_type=F32)
        total = term if total is None else total + term
    pairs = total.reshape(keep_ref.shape[0], 2, keep_ref.shape[1], total.shape[1])
    even, odd = pairs[:, 0], pairs[:, 1]
    mine = place_ref[1] == 0
    keep_ref[...] = jnp.where(mine, even, odd)
    send_ref[...] = jnp.where(mine, odd, even).astype(BF16)


def down_of(place, down, pieces, at, owners):
    experts, _, features = down.shape
    _, n_owner, rows, _ = pieces[0][0].shape
    flat, specs = [], []
    for p, group in enumerate(pieces):
        for piece in group:
            flat.append(piece)
            specs.append(
                pl.BlockSpec((1, owners, rows, piece.shape[3]), functools.partial(lambda q, i: (q, i, 0, 0), at[p]))
            )
    out = pl.BlockSpec((owners // 2, rows, features), lambda i: (i, 0, 0))
    return pl.pallas_call(
        functools.partial(down_kernel, experts),
        grid=(n_owner // owners,),
        in_specs=[
            pl.BlockSpec(memory_space=pltpu.SMEM),
            pl.BlockSpec(down.shape, lambda i: (0, 0, 0)),
            *specs,
        ],
        out_specs=[out, out],
        out_shape=[
            jax.ShapeDtypeStruct((n_owner // 2, rows, features), F32),
            jax.ShapeDtypeStruct((n_owner // 2, rows, features), BF16),
        ],
        compiler_params=params("arbitrary"),
        cost_estimate=pl.CostEstimate(
            flops=2 * n_owner * rows * down.size, bytes_accessed=n_owner * rows * (features * 3 + 2048), transcendentals=0
        ),
        name="down",
    )(place, down, *flat)


def around(array, axis):
    n = lax.axis_size(axis)
    got = {0: array}
    for shift in [1, n - 1, *range(2, n - 1)]:
        got[shift] = lax.ppermute(array, axis, [(i, (i + shift) % n) for i in range(n)])
    return [got[shift] for shift in range(n)]


def body(chunks, tokens, routes, route_logits, gain, w_gate, w_up, w_down):
    n_fs, n_tp = lax.axis_size("fs"), lax.axis_size("tp")
    experts, hidden_rows, features = w_down.shape
    count, depth = tokens.shape
    me = lax.axis_index("fs")
    expert = lax.axis_index("tp").astype(jnp.int32)
    parts = ((0, LANES), (LANES, hidden_rows - LANES))

    values = tokens.astype(F32)
    mean_square = jnp.mean(values * values, axis=-1, keepdims=True)
    normed = (values * lax.rsqrt(mean_square + 1e-06)).astype(BF16)
    first = jax.nn.sigmoid(route_logits[:, 0:1] - route_logits[:, 1:2])
    second = jax.nn.sigmoid(route_logits[:, 1:2] - route_logits[:, 0:1])
    names = lax.broadcasted_iota(jnp.int32, (count, LANES), 1)
    share = first * (routes[:, 0:1] == names).astype(F32)
    share = (share + second * (routes[:, 1:2] == names).astype(F32)).astype(BF16)
    rows = jnp.concatenate([normed, share], axis=1)
    gathered = lax.all_gather(rows, "fs", axis=0, tiled=True)
    gathered = gathered.reshape(n_fs, chunks, count // chunks, depth + LANES)

    packed = pack(gain, w_gate, w_up, parts, hidden_rows)
    received = []
    for piece in packed:
        e, blocks, size, lanes = piece.shape
        across = lax.all_to_all(piece.reshape(e, blocks * size, lanes), "tp", 0, 0, tiled=True)
        across = across.reshape(n_fs, size, lanes)
        received.append(lax.all_to_all(across, "fs", 0, 0, tiled=True))

    down_cast = w_down.astype(BF16)
    down_rows = lax.all_to_all(down_cast, "tp", 0, 0, tiled=True)
    down_served = jnp.swapaxes(down_rows, 0, 1).reshape(1, hidden_rows, n_tp * features)
    down_padded = jnp.pad(down_cast, ((0, 0), (0, len(parts) * LANES - hidden_rows), (0, 0)))

    place = jnp.stack([expert, (me % 2).astype(jnp.int32)])
    mine = expert[None]
    gates, ups, boths = zip(*(unpack(r, LANES) for r in received))
    early = around(hidden_of(mine, gathered, boths[0], depth, 0, chunks, 8), "tp")
    swap = [(i, i + 1 - 2 * (i % 2)) for i in range(n_fs)]
    columns = [list(range(c, n_fs, 2)) for c in range(2)]
    out = []
    for q in range(chunks):
        late = around(hidden_of(mine, gathered, boths[1], depth, q, 1, 8), "tp")
        keep, send = down_of(place, down_padded, [early, late], [q, 0], 8)
        summed = (keep + lax.ppermute(send, "fs", swap).astype(F32)).astype(BF16)
        spread = lax.all_to_all(summed, "fs", 0, 0, axis_index_groups=columns, tiled=True)
        out.append(jnp.sum(spread.astype(F32), axis=0).astype(BF16))
    mixed = jnp.concatenate(out, axis=0)
    gate_served = jnp.concatenate(gates, axis=0).T[None]
    up_served = jnp.concatenate(ups, axis=0).T[None]
    return gate_served, up_served, down_served, mixed


def solution(mesh):
    return jax.shard_map(
        functools.partial(body, 2),
        mesh=mesh,
        in_specs=(
            P(("grp", "fs"), None),
            P(("grp", "fs"), None),
            P(("grp", "fs"), None),
            P("fs"),
            P(None, "fs", "tp"),
            P(None, "fs", "tp"),
            P(None, "fs", "tp"),
        ),
        out_specs=(
            P(("grp", "tp"), None, "fs"),
            P(("grp", "tp"), None, "fs"),
            P(("grp", "tp"), "fs", None),
            P(("grp", "fs"), "tp"),
        ),
        check_vma=False,
    )
```

```python
import functools

import jax
import jax.numpy as jnp
from jax import lax
from jax.experimental import pallas as pl
from jax.experimental.pallas import tpu as pltpu
from jax.sharding import PartitionSpec as P

BF16, F32 = jnp.bfloat16, jnp.float32
LANES = 128
VMEM = 56 * 1024 * 1024


def params(*semantics):
    return pltpu.CompilerParams(dimension_semantics=semantics, vmem_limit_bytes=VMEM)


def pack_kernel(parts, width, place_ref, scale_ref, gate_ref, up_ref, first_ref, *late_refs):
    del place_ref
    both = jnp.concatenate([gate_ref[0], up_ref[0]], axis=0)
    columns = (both.T * scale_ref[...]).astype(BF16)
    blocks = columns.shape[0] // width
    for k in range(blocks):
        low, size = parts[0]
        first_ref[0, k] = columns[k * width + low : k * width + low + size]
    for shift, late_ref in enumerate(late_refs):

        @pl.when(pl.program_id(0) == shift)
        def _():
            low, size = parts[1]
            for k in range(blocks):
                late_ref[k] = columns[k * width + low : k * width + low + size]


def pack(place, gain, w_gate, w_up, parts, width):
    experts, rows, columns = w_gate.shape
    scale = jnp.concatenate([gain, gain])[None, :]
    blocks = columns // width
    chosen = lambda s, place_ref: (lax.rem(s + place_ref[0], experts), 0, 0)
    out = pl.pallas_call(
        functools.partial(pack_kernel, parts, width),
        grid_spec=pltpu.PrefetchScalarGridSpec(
            num_scalar_prefetch=1,
            grid=(experts,),
            in_specs=[
                pl.BlockSpec((1, 2 * rows), lambda s, place_ref: (0, 0)),
                pl.BlockSpec((1, rows, columns), chosen),
                pl.BlockSpec((1, rows, columns), chosen),
            ],
            out_specs=[
                pl.BlockSpec(
                    (1, blocks, parts[0][1], 2 * rows),
                    lambda s, place_ref: (lax.rem(s + place_ref[0], experts), 0, 0, 0),
                ),
                *[pl.BlockSpec((blocks, parts[1][1], 2 * rows), lambda s, place_ref: (0, 0, 0))] * experts,
            ],
        ),
        out_shape=[
            jax.ShapeDtypeStruct((experts, blocks, parts[0][1], 2 * rows), BF16),
            *[jax.ShapeDtypeStruct((blocks, parts[1][1], 2 * rows), BF16)] * experts,
        ],
        compiler_params=params("arbitrary"),
        cost_estimate=pl.CostEstimate(
            flops=experts * rows * columns * 1000, bytes_accessed=experts * rows * columns * 12, transcendentals=0
        ),
        name="pack",
    )(place, scale, w_gate, w_up)
    return out[0], out[1:]


def cast_kernel(place_ref, down_ref, padded_ref, *piece_refs):
    del place_ref
    rows = down_ref.shape[1]
    cast = down_ref[0].astype(BF16)
    padded_ref[0, :rows] = cast
    padded_ref[0, rows:] = jnp.zeros((padded_ref.shape[1] - rows, cast.shape[1]), BF16)
    for shift, piece_ref in enumerate(piece_refs):

        @pl.when(pl.program_id(0) == shift)
        def _():
            piece_ref[...] = cast


def cast_down(place, w_down, padded):
    experts, rows, features = w_down.shape
    out = pl.pallas_call(
        cast_kernel,
        grid_spec=pltpu.PrefetchScalarGridSpec(
            num_scalar_prefetch=1,
            grid=(experts,),
            in_specs=[pl.BlockSpec((1, rows, features), lambda s, p: (lax.rem(s + p[0], experts), 0, 0))],
            out_specs=[
                pl.BlockSpec((1, padded, features), lambda s, p: (lax.rem(s + p[0], experts), 0, 0)),
                *[pl.BlockSpec((rows, features), lambda s, p: (0, 0))] * experts,
            ],
        ),
        out_shape=[
            jax.ShapeDtypeStruct((experts, padded, features), BF16),
            *[jax.ShapeDtypeStruct((rows, features), BF16)] * experts,
        ],
        compiler_params=params("arbitrary"),
        cost_estimate=pl.CostEstimate(flops=w_down.size * 500, bytes_accessed=w_down.size * 8, transcendentals=0),
        name="cast_down",
    )(place, w_down)
    return out[0], out[1:]


def join_kernel(place_ref, *refs):
    del place_ref
    out_ref = refs[-1]
    for shift, ref in enumerate(refs[:-1]):

        @pl.when(pl.program_id(0) == shift)
        def _():
            out_ref[...] = ref[...]


def join(place, pieces, dim):
    n, dims = len(pieces), pieces[0].shape
    spot = lambda s, p: tuple(lax.rem(p[0] + n - s, n) if d == dim else 0 for d in range(len(dims)))
    whole = tuple(size * n if d == dim else size for d, size in enumerate(dims))
    return pl.pallas_call(
        join_kernel,
        grid_spec=pltpu.PrefetchScalarGridSpec(
            num_scalar_prefetch=1,
            grid=(n,),
            in_specs=[pl.BlockSpec(dims, lambda s, p: (0,) * len(dims))] * n,
            out_specs=pl.BlockSpec(dims, spot),
        ),
        out_shape=jax.ShapeDtypeStruct(whole, BF16),
        compiler_params=params("arbitrary"),
        cost_estimate=pl.CostEstimate(flops=pieces[0].size * n * 500, bytes_accessed=pieces[0].size * n * 4, transcendentals=0),
        name="join",
    )(place, *pieces)


def unpack_kernel(size, recv_ref, gate_ref, up_ref, both_ref):
    half = recv_ref.shape[2] // 2
    pad = both_ref.shape[0] // 2 - size
    if pad:
        zeros = jnp.zeros((pad, both_ref.shape[1]), BF16)
        both_ref[size : size + pad] = zeros
        both_ref[size + pad + size :] = zeros
    for k in range(recv_ref.shape[0] // 2):
        one, two = recv_ref[2 * k], recv_ref[2 * k + 1]
        at = slice(k * 2 * half, (k + 1) * 2 * half)
        gate = jnp.concatenate([one[:, :half], two[:, :half]], axis=1)
        up = jnp.concatenate([one[:, half:], two[:, half:]], axis=1)
        gate_ref[:, at] = gate
        up_ref[:, at] = up
        both_ref[0:size, at] = gate
        both_ref[size + pad : size + pad + size, at] = up


def unpack(recv, padded):
    count, size, lanes = recv.shape
    width = count * lanes // 2
    return pl.pallas_call(
        functools.partial(unpack_kernel, size),
        in_specs=[pl.BlockSpec(memory_space=pltpu.VMEM)],
        out_specs=[pl.BlockSpec(memory_space=pltpu.VMEM)] * 3,
        out_shape=[
            jax.ShapeDtypeStruct((size, width), BF16),
            jax.ShapeDtypeStruct((size, width), BF16),
            jax.ShapeDtypeStruct((2 * padded, width), BF16),
        ],
        compiler_params=params(),
        cost_estimate=pl.CostEstimate(flops=count * size * lanes * 40, bytes_accessed=count * size * lanes * 6, transcendentals=0),
        name="unpack",
    )(recv)


def hidden_kernel(depth, expert_ref, tokens_ref, both_ref, out_ref):
    owners, rows = tokens_ref.shape[0], tokens_ref.shape[2]
    block = tokens_ref[...].reshape(owners * rows, tokens_ref.shape[3])
    acts = lax.dot_general(
        block[:, :depth], both_ref[...], (((1,), (1,)), ((), ())), preferred_element_type=F32
    )
    shares = block[:, depth:].astype(F32)
    lane = lax.broadcasted_iota(jnp.int32, shares.shape, 1)
    share = jnp.sum(jnp.where(lane == expert_ref[0], shares, 0.0), axis=1, keepdims=True)
    half = acts.shape[1] // 2
    gate, up = acts[:, :half], acts[:, half:]
    hidden = gate / (1.0 + jnp.exp(-gate)) * up * share
    out_ref[...] = hidden.astype(BF16).reshape(1, owners, rows, half)


def hidden_of(expert, tokens, both, depth, first, count, owners):
    n_owner, _, rows, wide = tokens.shape
    half = both.shape[0] // 2
    work = count * n_owner * rows
    return pl.pallas_call(
        functools.partial(hidden_kernel, depth),
        grid=(count, n_owner // owners),
        in_specs=[
            pl.BlockSpec(memory_space=pltpu.SMEM),
            pl.BlockSpec((owners, 1, rows, wide), lambda q, i: (i, q + first, 0, 0)),
            pl.BlockSpec(both.shape, lambda q, i: (0, 0)),
        ],
        out_specs=pl.BlockSpec((1, owners, rows, half), lambda q, i: (q, i, 0, 0)),
        out_shape=jax.ShapeDtypeStruct((count, n_owner, rows, half), BF16),
        compiler_params=params("arbitrary", "arbitrary"),
        cost_estimate=pl.CostEstimate(
            flops=2 * work * depth * 2 * half, bytes_accessed=work * wide * 2 + both.size * 2, transcendentals=work * half
        ),
        name="hidden",
    )(expert, tokens, both)


def down_kernel(experts, place_ref, down_ref, *refs):
    parts, (keep_ref, send_ref) = refs[:-2], refs[-2:]
    per = len(parts) // experts
    total = None
    for shift in range(experts):
        pieces = []
        for p in range(per):
            r = parts[p * experts + shift]
            pieces.append(r[...].reshape(-1, r.shape[-1]))
        source = lax.rem(place_ref[0] + experts - shift, experts)
        left = jnp.concatenate(pieces, axis=1) if per > 1 else pieces[0]
        term = jnp.dot(left, down_ref[source], preferred_element_type=F32)
        total = term if total is None else total + term
    pairs = total.reshape(keep_ref.shape[0], 2, keep_ref.shape[1], total.shape[1])
    even, odd = pairs[:, 0], pairs[:, 1]
    mine = place_ref[1] == 0
    keep_ref[...] = jnp.where(mine, even, odd)
    send_ref[...] = jnp.where(mine, odd, even).astype(BF16)


def down_of(place, down, pieces, at, owners):
    experts, _, features = down.shape
    _, n_owner, rows, _ = pieces[0][0].shape
    flat, specs = [], []
    for p, group in enumerate(pieces):
        for piece in group:
            flat.append(piece)
            specs.append(
                pl.BlockSpec((1, owners, rows, piece.shape[3]), functools.partial(lambda q, i: (q, i, 0, 0), at[p]))
            )
    out = pl.BlockSpec((owners // 2, rows, features), lambda i: (i, 0, 0))
    return pl.pallas_call(
        functools.partial(down_kernel, experts),
        grid=(n_owner // owners,),
        in_specs=[
            pl.BlockSpec(memory_space=pltpu.SMEM),
            pl.BlockSpec(down.shape, lambda i: (0, 0, 0)),
            *specs,
        ],
        out_specs=[out, out],
        out_shape=[
            jax.ShapeDtypeStruct((n_owner // 2, rows, features), F32),
            jax.ShapeDtypeStruct((n_owner // 2, rows, features), BF16),
        ],
        compiler_params=params("arbitrary"),
        cost_estimate=pl.CostEstimate(
            flops=2 * n_owner * rows * down.size, bytes_accessed=n_owner * rows * (features * 3 + 2048), transcendentals=0
        ),
        name="down",
    )(place, down, *flat)


def around(array, axis):
    n = lax.axis_size(axis)
    got = {0: array}
    for shift in [1, n - 1, *range(2, n - 1)]:
        got[shift] = lax.ppermute(array, axis, [(i, (i + shift) % n) for i in range(n)])
    return [got[shift] for shift in range(n)]


def dealt(pieces, axis):
    n = lax.axis_size(axis)
    got = {0: pieces[0]}
    for shift in [1, n - 1, *range(2, n - 1)]:
        got[shift] = lax.ppermute(pieces[shift], axis, [(i, (i + shift) % n) for i in range(n)])
    return [got[shift] for shift in range(n)]


def body(chunks, tokens, routes, route_logits, gain, w_gate, w_up, w_down):
    n_fs, n_tp = lax.axis_size("fs"), lax.axis_size("tp")
    experts, hidden_rows, features = w_down.shape
    count, depth = tokens.shape
    me = lax.axis_index("fs")
    expert = lax.axis_index("tp").astype(jnp.int32)
    parts = ((0, LANES), (LANES, hidden_rows - LANES))

    values = tokens.astype(F32)
    mean_square = jnp.mean(values * values, axis=-1, keepdims=True)
    normed = (values * lax.rsqrt(mean_square + 1e-06)).astype(BF16)
    first = jax.nn.sigmoid(route_logits[:, 0:1] - route_logits[:, 1:2])
    second = jax.nn.sigmoid(route_logits[:, 1:2] - route_logits[:, 0:1])
    names = lax.broadcasted_iota(jnp.int32, (count, LANES), 1)
    share = first * (routes[:, 0:1] == names).astype(F32)
    share = (share + second * (routes[:, 1:2] == names).astype(F32)).astype(BF16)
    rows = jnp.concatenate([normed, share], axis=1)
    gathered = lax.all_gather(rows, "fs", axis=0, tiled=True)
    gathered = gathered.reshape(n_fs, chunks, count // chunks, depth + LANES)

    place = jnp.stack([expert, (me % 2).astype(jnp.int32)])
    mine = expert[None]
    first_part, late_parts = pack(place, gain, w_gate, w_up, parts, hidden_rows)
    first_part = first_part.reshape(n_tp, -1, first_part.shape[3])
    across = lax.all_to_all(first_part, "tp", 0, 0, tiled=True).reshape(n_fs, -1, first_part.shape[2])
    received = lax.all_to_all(across, "fs", 0, 0, tiled=True)
    late_across = join(place, dealt(late_parts, "tp"), 0)
    late_across, received = lax.optimization_barrier((late_across, received))
    late_received = lax.all_to_all(late_across, "fs", 0, 0, tiled=True)

    down_padded, down_pieces = cast_down(place, w_down, len(parts) * LANES)
    down_served = join(place, dealt(down_pieces, "tp"), 1)[None]

    gate_a, up_a, both_a = unpack(received, LANES)
    early = around(hidden_of(mine, gathered, both_a, depth, 0, chunks, 8), "tp")
    late_received, early = lax.optimization_barrier((late_received, early))
    gate_b, up_b, both_b = unpack(late_received, LANES)
    gates, ups = (gate_a, gate_b), (up_a, up_b)
    swap = [(i, i + 1 - 2 * (i % 2)) for i in range(n_fs)]
    columns = [list(range(c, n_fs, 2)) for c in range(2)]
    lates = [around(hidden_of(mine, gathered, both_b, depth, q, 1, 8), "tp") for q in range(chunks)]
    out = []
    for q in range(chunks):
        keep, send = down_of(place, down_padded, [early, lates[q]], [q, 0], 8)
        summed = (keep + lax.ppermute(send, "fs", swap).astype(F32)).astype(BF16)
        spread = lax.all_to_all(summed, "fs", 0, 0, axis_index_groups=columns, tiled=True)
        out.append(jnp.sum(spread.astype(F32), axis=0).astype(BF16))
    mixed = jnp.concatenate(out, axis=0)
    gate_served = jnp.concatenate(gates, axis=0).T[None]
    up_served = jnp.concatenate(ups, axis=0).T[None]
    return gate_served, up_served, down_served, mixed


def solution(mesh):
    return jax.shard_map(
        functools.partial(body, 2),
        mesh=mesh,
        in_specs=(
            P(("grp", "fs"), None),
            P(("grp", "fs"), None),
            P(("grp", "fs"), None),
            P("fs"),
            P(None, "fs", "tp"),
            P(None, "fs", "tp"),
            P(None, "fs", "tp"),
        ),
        out_specs=(
            P(("grp", "tp"), None, "fs"),
            P(("grp", "tp"), None, "fs"),
            P(("grp", "tp"), "fs", None),
            P(("grp", "fs"), "tp"),
        ),
        check_vma=False,
    )
```

```python
import functools

import jax
import jax.numpy as jnp
from jax import lax
from jax.experimental import pallas as pl
from jax.experimental.pallas import tpu as pltpu
from jax.sharding import PartitionSpec as P

BF16, F32 = jnp.bfloat16, jnp.float32
LANES = 128
VMEM = 56 * 1024 * 1024


def params(*semantics):
    return pltpu.CompilerParams(dimension_semantics=semantics, vmem_limit_bytes=VMEM)


def pack_kernel(parts, width, place_ref, scale_ref, gate_ref, up_ref, first_ref, *late_refs):
    del place_ref
    both = jnp.concatenate([gate_ref[0], up_ref[0]], axis=0)
    columns = (both.T * scale_ref[...]).astype(BF16)
    blocks = columns.shape[0] // width
    for k in range(blocks):
        low, size = parts[0]
        first_ref[0, k] = columns[k * width + low : k * width + low + size]
    for shift, late_ref in enumerate(late_refs):

        @pl.when(pl.program_id(0) == shift)
        def _():
            low, size = parts[1]
            for k in range(blocks):
                late_ref[k] = columns[k * width + low : k * width + low + size]


def pack(place, gain, w_gate, w_up, parts, width):
    experts, rows, columns = w_gate.shape
    scale = jnp.concatenate([gain, gain])[None, :]
    blocks = columns // width
    chosen = lambda s, place_ref: (lax.rem(s + place_ref[0], experts), 0, 0)
    out = pl.pallas_call(
        functools.partial(pack_kernel, parts, width),
        grid_spec=pltpu.PrefetchScalarGridSpec(
            num_scalar_prefetch=1,
            grid=(experts,),
            in_specs=[
                pl.BlockSpec((1, 2 * rows), lambda s, place_ref: (0, 0)),
                pl.BlockSpec((1, rows, columns), chosen),
                pl.BlockSpec((1, rows, columns), chosen),
            ],
            out_specs=[
                pl.BlockSpec(
                    (1, blocks, parts[0][1], 2 * rows),
                    lambda s, place_ref: (lax.rem(s + place_ref[0], experts), 0, 0, 0),
                ),
                *[pl.BlockSpec((blocks, parts[1][1], 2 * rows), lambda s, place_ref: (0, 0, 0))] * experts,
            ],
        ),
        out_shape=[
            jax.ShapeDtypeStruct((experts, blocks, parts[0][1], 2 * rows), BF16),
            *[jax.ShapeDtypeStruct((blocks, parts[1][1], 2 * rows), BF16)] * experts,
        ],
        compiler_params=params("arbitrary"),
        cost_estimate=pl.CostEstimate(
            flops=experts * rows * columns * 1000, bytes_accessed=experts * rows * columns * 12, transcendentals=0
        ),
        name="pack",
    )(place, scale, w_gate, w_up)
    return out[0], out[1:]


def cast_kernel(place_ref, down_ref, padded_ref, *piece_refs):
    del place_ref
    rows = down_ref.shape[1]
    cast = down_ref[0].astype(BF16)
    padded_ref[0, :rows] = cast
    padded_ref[0, rows:] = jnp.zeros((padded_ref.shape[1] - rows, cast.shape[1]), BF16)
    for shift, piece_ref in enumerate(piece_refs):

        @pl.when(pl.program_id(0) == shift)
        def _():
            piece_ref[...] = cast


def cast_down(place, w_down, padded):
    experts, rows, features = w_down.shape
    out = pl.pallas_call(
        cast_kernel,
        grid_spec=pltpu.PrefetchScalarGridSpec(
            num_scalar_prefetch=1,
            grid=(experts,),
            in_specs=[pl.BlockSpec((1, rows, features), lambda s, p: (lax.rem(s + p[0], experts), 0, 0))],
            out_specs=[
                pl.BlockSpec((1, padded, features), lambda s, p: (lax.rem(s + p[0], experts), 0, 0)),
                *[pl.BlockSpec((rows, features), lambda s, p: (0, 0))] * experts,
            ],
        ),
        out_shape=[
            jax.ShapeDtypeStruct((experts, padded, features), BF16),
            *[jax.ShapeDtypeStruct((rows, features), BF16)] * experts,
        ],
        compiler_params=params("arbitrary"),
        cost_estimate=pl.CostEstimate(flops=w_down.size * 500, bytes_accessed=w_down.size * 8, transcendentals=0),
        name="cast_down",
    )(place, w_down)
    return out[0], out[1:]


def join_kernel(place_ref, *refs):
    del place_ref
    out_ref = refs[-1]
    for shift, ref in enumerate(refs[:-1]):

        @pl.when(pl.program_id(0) == shift)
        def _():
            out_ref[...] = ref[...]


def join(place, pieces, dim):
    n, dims = len(pieces), pieces[0].shape
    spot = lambda s, p: tuple(lax.rem(p[0] + n - s, n) if d == dim else 0 for d in range(len(dims)))
    whole = tuple(size * n if d == dim else size for d, size in enumerate(dims))
    return pl.pallas_call(
        join_kernel,
        grid_spec=pltpu.PrefetchScalarGridSpec(
            num_scalar_prefetch=1,
            grid=(n,),
            in_specs=[pl.BlockSpec(dims, lambda s, p: (0,) * len(dims))] * n,
            out_specs=pl.BlockSpec(dims, spot),
        ),
        out_shape=jax.ShapeDtypeStruct(whole, BF16),
        compiler_params=params("arbitrary"),
        cost_estimate=pl.CostEstimate(flops=pieces[0].size * n * 500, bytes_accessed=pieces[0].size * n * 4, transcendentals=0),
        name="join",
    )(place, *pieces)


def unpack_kernel(size, recv_ref, gate_ref, up_ref, both_ref):
    half = recv_ref.shape[2] // 2
    pad = both_ref.shape[0] // 2 - size
    if pad:
        zeros = jnp.zeros((pad, both_ref.shape[1]), BF16)
        both_ref[size : size + pad] = zeros
        both_ref[size + pad + size :] = zeros
    for k in range(recv_ref.shape[0] // 2):
        one, two = recv_ref[2 * k], recv_ref[2 * k + 1]
        at = slice(k * 2 * half, (k + 1) * 2 * half)
        gate = jnp.concatenate([one[:, :half], two[:, :half]], axis=1)
        up = jnp.concatenate([one[:, half:], two[:, half:]], axis=1)
        gate_ref[:, at] = gate
        up_ref[:, at] = up
        both_ref[0:size, at] = gate
        both_ref[size + pad : size + pad + size, at] = up


def unpack(recv, padded):
    count, size, lanes = recv.shape
    width = count * lanes // 2
    return pl.pallas_call(
        functools.partial(unpack_kernel, size),
        in_specs=[pl.BlockSpec(memory_space=pltpu.VMEM)],
        out_specs=[pl.BlockSpec(memory_space=pltpu.VMEM)] * 3,
        out_shape=[
            jax.ShapeDtypeStruct((size, width), BF16),
            jax.ShapeDtypeStruct((size, width), BF16),
            jax.ShapeDtypeStruct((2 * padded, width), BF16),
        ],
        compiler_params=params(),
        cost_estimate=pl.CostEstimate(flops=count * size * lanes * 40, bytes_accessed=count * size * lanes * 6, transcendentals=0),
        name="unpack",
    )(recv)


def hidden_kernel(depth, n_tp, first, place_ref, early_ref, late_ref, *refs):
    token_refs, (out_ref, block_ref) = refs[:-2], refs[-2:]
    quarter, core = pl.program_id(0) + first, pl.program_id(1)
    shift = lax.rem(place_ref[0] + n_tp - quarter, n_tp)
    other = jnp.where(core == place_ref[1], 0, 1)
    for k, token_ref in enumerate(token_refs):

        @pl.when(2 * shift + other == k)
        def _():
            block_ref[...] = token_ref[...]

    tokens = block_ref[:, :depth]
    shares = block_ref[:, depth:].astype(F32)
    lane = lax.broadcasted_iota(jnp.int32, shares.shape, 1)
    share = jnp.sum(jnp.where(lane == place_ref[0], shares, 0.0), axis=1, keepdims=True)
    at = 0
    for both_ref in (early_ref, late_ref):
        acts = lax.dot_general(tokens, both_ref[...], (((1,), (1,)), ((), ())), preferred_element_type=F32)
        half = acts.shape[1] // 2
        gate, up = acts[:, :half], acts[:, half:]
        hidden = gate / (1.0 + jnp.exp(-gate)) * up * share
        out_ref[0, 0, :, at : at + half] = hidden.astype(BF16)
        at += half


def hidden_of(place, tokens, boths, depth, first, count):
    n_tp = len(tokens) // 2
    rows, wide = tokens[0].shape
    half = sum(both.shape[0] for both in boths) // 2
    work = count * 2 * rows
    vmem = pl.BlockSpec(memory_space=pltpu.VMEM)
    return pl.pallas_call(
        functools.partial(hidden_kernel, depth, n_tp, first),
        grid=(count, 2),
        in_specs=[pl.BlockSpec(memory_space=pltpu.SMEM), vmem, vmem, *[vmem] * len(tokens)],
        out_specs=pl.BlockSpec((1, 1, rows, half), lambda q, c: (q, c, 0, 0)),
        out_shape=jax.ShapeDtypeStruct((count, 2, rows, half), BF16),
        scratch_shapes=[pltpu.VMEM((rows, wide), BF16)],
        compiler_params=params("arbitrary", "arbitrary"),
        cost_estimate=pl.CostEstimate(
            flops=2 * work * depth * 2 * half, bytes_accessed=work * wide * 2, transcendentals=work * half
        ),
        name="hidden",
    )(place, *boths, *tokens)


def down_kernel(place_ref, down_ref, *refs):
    parts, (keep_ref, send_ref) = refs[:-2], refs[-2:]
    experts = len(parts)
    total = None
    for shift, part_ref in enumerate(parts):
        left = part_ref[0].reshape(-1, part_ref.shape[3])
        source = lax.rem(place_ref[0] + experts - shift, experts)
        term = jnp.dot(left, down_ref[source], preferred_element_type=F32)
        total = term if total is None else total + term
    rows = total.shape[0] // 2
    mine = place_ref[1] == 0
    even, odd = total[:rows], total[rows:]
    keep = jnp.where(mine, even, odd)
    send = jnp.where(mine, odd, even).astype(BF16)
    keep_ref[...] = keep.reshape(keep_ref.shape)
    send_ref[...] = send.reshape(send_ref.shape)


def down_of(place, down, pieces, n_z):
    features = down.shape[2]
    count, _, rows, width = pieces[0].shape
    out = pl.BlockSpec((n_z, 1, rows // n_z, features), lambda q: (0, q, 0, 0))
    shape = (n_z, count, rows // n_z, features)
    return pl.pallas_call(
        down_kernel,
        grid=(count,),
        in_specs=[
            pl.BlockSpec(memory_space=pltpu.SMEM),
            pl.BlockSpec(down.shape, lambda q: (0, 0, 0)),
            *[pl.BlockSpec((1, 2, rows, width), lambda q: (q, 0, 0, 0))] * len(pieces),
        ],
        out_specs=[out, out],
        out_shape=[jax.ShapeDtypeStruct(shape, F32), jax.ShapeDtypeStruct(shape, BF16)],
        compiler_params=params("arbitrary"),
        cost_estimate=pl.CostEstimate(
            flops=4 * count * rows * down.size, bytes_accessed=count * rows * 2 * (features * 3 + 2048), transcendentals=0
        ),
        name="down",
    )(place, down, *pieces)


def held_kernel(in_ref, out_ref):
    out_ref[...] = in_ref[...]


def held(array):
    vmem = pl.BlockSpec(memory_space=pltpu.VMEM)
    return pl.pallas_call(
        held_kernel,
        in_specs=[vmem],
        out_specs=vmem,
        out_shape=jax.ShapeDtypeStruct(array.shape, array.dtype),
        compiler_params=params(),
        cost_estimate=pl.CostEstimate(flops=array.size * 500, bytes_accessed=array.size * 4, transcendentals=0),
        name="held",
    )(array)


def around(array, axis):
    n = lax.axis_size(axis)
    got = {0: array}
    for shift in [1, n - 1, *range(2, n - 1)]:
        got[shift] = lax.ppermute(array, axis, [(i, (i + shift) % n) for i in range(n)])
    return [got[shift] for shift in range(n)]


def dealt(pieces, axis):
    n = lax.axis_size(axis)
    got = {0: pieces[0]}
    for shift in [1, n - 1, *range(2, n - 1)]:
        got[shift] = lax.ppermute(pieces[shift], axis, [(i, (i + shift) % n) for i in range(n)])
    return [got[shift] for shift in range(n)]


def body(chunks, tokens, routes, route_logits, gain, w_gate, w_up, w_down):
    n_fs, n_tp = lax.axis_size("fs"), lax.axis_size("tp")
    _, hidden_rows, features = w_down.shape
    count, depth = tokens.shape
    me = lax.axis_index("fs")
    expert = lax.axis_index("tp").astype(jnp.int32)
    place = jnp.stack([expert, (me % 2).astype(jnp.int32)])
    parts = ((0, LANES), (LANES, hidden_rows - LANES))
    swap = [(i, i + 1 - 2 * (i % 2)) for i in range(n_fs)]
    columns = [list(range(c, n_fs, 2)) for c in range(2)]
    n_z = n_fs // 2

    some = count // n_tp
    tokens, routes, route_logits = (
        lax.dynamic_slice_in_dim(a, expert * some, some) for a in (tokens, routes, route_logits)
    )
    values = tokens.astype(F32)
    mean_square = jnp.mean(values * values, axis=-1, keepdims=True)
    normed = (values * lax.rsqrt(mean_square + 1e-06)).astype(BF16)
    first = jax.nn.sigmoid(route_logits[:, 0:1] - route_logits[:, 1:2])
    second = jax.nn.sigmoid(route_logits[:, 1:2] - route_logits[:, 0:1])
    names = lax.broadcasted_iota(jnp.int32, (some, LANES), 1)
    share = first * (routes[:, 0:1] == names).astype(F32)
    share = (share + second * (routes[:, 1:2] == names).astype(F32)).astype(BF16)
    rows = jnp.concatenate([normed, share], axis=1)
    rows, place = lax.optimization_barrier((rows, place))
    quarter = lax.all_gather(rows, "fs", axis=0, axis_index_groups=columns, tiled=True)
    first_part, late_parts = pack(place, gain, w_gate, w_up, parts, hidden_rows)
    first_part = first_part.reshape(n_tp, -1, first_part.shape[3])
    across = lax.all_to_all(first_part, "tp", 0, 0, tiled=True).reshape(n_fs, -1, first_part.shape[2])
    received = lax.all_to_all(across, "fs", 0, 0, tiled=True)
    late_across = join(place, dealt(late_parts, "tp"), 0)
    late_across, received = lax.optimization_barrier((late_across, received))
    late_received = lax.all_to_all(late_across, "fs", 0, 0, tiled=True)

    quarter = held(quarter)
    quarters = around(quarter, "tp")
    all_tokens = []
    for piece in quarters:
        all_tokens += [piece, lax.ppermute(piece, "fs", swap)]

    down_padded, down_pieces = cast_down(place, w_down, len(parts) * LANES)
    down_served = join(place, dealt(down_pieces, "tp"), 1)[None]

    gate_a, up_a, both_a = unpack(received, LANES)
    gate_b, up_b, both_b = unpack(late_received, LANES)
    gates, ups = (gate_a, gate_b), (up_a, up_b)
    per = n_tp // chunks
    hiddens = [hidden_of(place, all_tokens, (both_a, both_b), depth, q * per, per) for q in range(chunks)]
    gathered = []
    for hidden in hiddens:
        gathered.append(around(hidden, "tp"))
    *gathered[0], hiddens[1] = lax.optimization_barrier((*gathered[0], hiddens[1]))
    gathered[1][0] = hiddens[1]
    out = []
    for q in range(chunks):
        keep, send = down_of(place, down_padded, gathered[q], n_z)
        summed = (keep + lax.ppermute(send, "fs", swap).astype(F32)).astype(BF16)
        summed = summed.reshape(n_z, per * some, features)
        spread = lax.all_to_all(summed, "fs", 0, 0, axis_index_groups=columns, tiled=True)
        out.append(jnp.sum(spread.astype(F32), axis=0).astype(BF16))
    mixed = jnp.concatenate(out, axis=0)
    gate_served = jnp.concatenate(gates, axis=0).T[None]
    up_served = jnp.concatenate(ups, axis=0).T[None]
    return gate_served, up_served, down_served, mixed


def layer(chunks, *args):
    return body(chunks, *args)


def solution(mesh):
    return jax.shard_map(
        functools.partial(layer, 2),
        mesh=mesh,
        in_specs=(
            P(("grp", "fs"), None),
            P(("grp", "fs"), None),
            P(("grp", "fs"), None),
            P("fs"),
            P(None, "fs", "tp"),
            P(None, "fs", "tp"),
            P(None, "fs", "tp"),
        ),
        out_specs=(
            P(("grp", "tp"), None, "fs"),
            P(("grp", "tp"), None, "fs"),
            P(("grp", "tp"), "fs", None),
            P(("grp", "fs"), "tp"),
        ),
        check_vma=False,
    )
```

```python
import functools

import jax
import jax.numpy as jnp
from jax import lax
from jax.experimental import pallas as pl
from jax.experimental.pallas import tpu as pltpu
from jax.sharding import PartitionSpec as P

BF16, F32 = jnp.bfloat16, jnp.float32
LANES = 128
VMEM = 56 * 1024 * 1024


def params(*semantics):
    return pltpu.CompilerParams(dimension_semantics=semantics, vmem_limit_bytes=VMEM)


def pack_kernel(parts, width, place_ref, scale_ref, gate_ref, up_ref, first_ref, *late_refs):
    del place_ref
    both = jnp.concatenate([gate_ref[0], up_ref[0]], axis=0)
    columns = (both.T * scale_ref[...]).astype(BF16)
    blocks = columns.shape[0] // width
    for k in range(blocks):
        low, size = parts[0]
        first_ref[0, k] = columns[k * width + low : k * width + low + size]
    for shift, late_ref in enumerate(late_refs):

        @pl.when(pl.program_id(0) == shift)
        def _():
            low, size = parts[1]
            for k in range(blocks):
                late_ref[k] = columns[k * width + low : k * width + low + size]


def pack(place, gain, w_gate, w_up, parts, width):
    experts, rows, columns = w_gate.shape
    scale = jnp.concatenate([gain, gain])[None, :]
    blocks = columns // width
    chosen = lambda s, place_ref: (lax.rem(s + place_ref[0], experts), 0, 0)
    out = pl.pallas_call(
        functools.partial(pack_kernel, parts, width),
        grid_spec=pltpu.PrefetchScalarGridSpec(
            num_scalar_prefetch=1,
            grid=(experts,),
            in_specs=[
                pl.BlockSpec((1, 2 * rows), lambda s, place_ref: (0, 0)),
                pl.BlockSpec((1, rows, columns), chosen),
                pl.BlockSpec((1, rows, columns), chosen),
            ],
            out_specs=[
                pl.BlockSpec(
                    (1, blocks, parts[0][1], 2 * rows),
                    lambda s, place_ref: (lax.rem(s + place_ref[0], experts), 0, 0, 0),
                ),
                *[pl.BlockSpec((blocks, parts[1][1], 2 * rows), lambda s, place_ref: (0, 0, 0))] * experts,
            ],
        ),
        out_shape=[
            jax.ShapeDtypeStruct((experts, blocks, parts[0][1], 2 * rows), BF16),
            *[jax.ShapeDtypeStruct((blocks, parts[1][1], 2 * rows), BF16)] * experts,
        ],
        compiler_params=params("arbitrary"),
        cost_estimate=pl.CostEstimate(
            flops=experts * rows * columns * 1000, bytes_accessed=experts * rows * columns * 12, transcendentals=0
        ),
        name="pack",
    )(place, scale, w_gate, w_up)
    return out[0], out[1:]


def cast_kernel(place_ref, down_ref, padded_ref, *piece_refs):
    del place_ref
    rows = down_ref.shape[1]
    cast = down_ref[0].astype(BF16)
    padded_ref[0, :rows] = cast
    padded_ref[0, rows:] = jnp.zeros((padded_ref.shape[1] - rows, cast.shape[1]), BF16)
    for shift, piece_ref in enumerate(piece_refs):

        @pl.when(pl.program_id(0) == shift)
        def _():
            piece_ref[...] = cast


def cast_down(place, w_down, padded):
    experts, rows, features = w_down.shape
    out = pl.pallas_call(
        cast_kernel,
        grid_spec=pltpu.PrefetchScalarGridSpec(
            num_scalar_prefetch=1,
            grid=(experts,),
            in_specs=[pl.BlockSpec((1, rows, features), lambda s, p: (lax.rem(s + p[0], experts), 0, 0))],
            out_specs=[
                pl.BlockSpec((1, padded, features), lambda s, p: (lax.rem(s + p[0], experts), 0, 0)),
                *[pl.BlockSpec((rows, features), lambda s, p: (0, 0))] * experts,
            ],
        ),
        out_shape=[
            jax.ShapeDtypeStruct((experts, padded, features), BF16),
            *[jax.ShapeDtypeStruct((rows, features), BF16)] * experts,
        ],
        compiler_params=params("arbitrary"),
        cost_estimate=pl.CostEstimate(flops=w_down.size * 500, bytes_accessed=w_down.size * 8, transcendentals=0),
        name="cast_down",
    )(place, w_down)
    return out[0], out[1:]


def join_kernel(place_ref, *refs):
    del place_ref
    out_ref = refs[-1]
    for shift, ref in enumerate(refs[:-1]):

        @pl.when(pl.program_id(0) == shift)
        def _():
            out_ref[...] = ref[...]


def join(place, pieces, dim):
    n, dims = len(pieces), pieces[0].shape
    spot = lambda s, p: tuple(lax.rem(p[0] + n - s, n) if d == dim else 0 for d in range(len(dims)))
    whole = tuple(size * n if d == dim else size for d, size in enumerate(dims))
    return pl.pallas_call(
        join_kernel,
        grid_spec=pltpu.PrefetchScalarGridSpec(
            num_scalar_prefetch=1,
            grid=(n,),
            in_specs=[pl.BlockSpec(dims, lambda s, p: (0,) * len(dims))] * n,
            out_specs=pl.BlockSpec(dims, spot),
        ),
        out_shape=jax.ShapeDtypeStruct(whole, BF16),
        compiler_params=params("arbitrary"),
        cost_estimate=pl.CostEstimate(flops=pieces[0].size * n * 500, bytes_accessed=pieces[0].size * n * 4, transcendentals=0),
        name="join",
    )(place, *pieces)


def unpack_kernel(size, recv_ref, gate_ref, up_ref, both_ref):
    half = recv_ref.shape[2] // 2
    pad = both_ref.shape[0] // 2 - size
    if pad:
        zeros = jnp.zeros((pad, both_ref.shape[1]), BF16)
        both_ref[size : size + pad] = zeros
        both_ref[size + pad + size :] = zeros
    for k in range(recv_ref.shape[0] // 2):
        one, two = recv_ref[2 * k], recv_ref[2 * k + 1]
        at = slice(k * 2 * half, (k + 1) * 2 * half)
        gate = jnp.concatenate([one[:, :half], two[:, :half]], axis=1)
        up = jnp.concatenate([one[:, half:], two[:, half:]], axis=1)
        gate_ref[:, at] = gate
        up_ref[:, at] = up
        both_ref[0:size, at] = gate
        both_ref[size + pad : size + pad + size, at] = up


def unpack(recv, padded):
    count, size, lanes = recv.shape
    width = count * lanes // 2
    return pl.pallas_call(
        functools.partial(unpack_kernel, size),
        in_specs=[pl.BlockSpec(memory_space=pltpu.VMEM)],
        out_specs=[pl.BlockSpec(memory_space=pltpu.VMEM)] * 3,
        out_shape=[
            jax.ShapeDtypeStruct((size, width), BF16),
            jax.ShapeDtypeStruct((size, width), BF16),
            jax.ShapeDtypeStruct((2 * padded, width), BF16),
        ],
        compiler_params=params(),
        cost_estimate=pl.CostEstimate(flops=count * size * lanes * 40, bytes_accessed=count * size * lanes * 6, transcendentals=0),
        name="unpack",
    )(recv)


def hidden_kernel(depth, n_tp, first, n_parts, place_ref, *refs):
    both_refs, token_refs, (out_ref, block_ref) = refs[:n_parts], refs[n_parts:-2], refs[-2:]
    quarter, core = pl.program_id(0) + first, pl.program_id(1)
    shift = lax.rem(place_ref[0] + n_tp - quarter, n_tp)
    other = jnp.where(core == place_ref[1], 0, 1)
    for k, token_ref in enumerate(token_refs):

        @pl.when(2 * shift + other == k)
        def _():
            block_ref[...] = token_ref[...]

    tokens = block_ref[:, :depth]
    shares = block_ref[:, depth:].astype(F32)
    lane = lax.broadcasted_iota(jnp.int32, shares.shape, 1)
    share = jnp.sum(jnp.where(lane == place_ref[0], shares, 0.0), axis=1, keepdims=True)
    at = 0
    for both_ref in both_refs:
        acts = lax.dot_general(tokens, both_ref[...], (((1,), (1,)), ((), ())), preferred_element_type=F32)
        half = acts.shape[1] // 2
        gate, up = acts[:, :half], acts[:, half:]
        hidden = gate / (1.0 + jnp.exp(-gate)) * up * share
        out_ref[0, 0, :, at : at + half] = hidden.astype(BF16)
        at += half


def hidden_of(place, tokens, boths, depth, first, count):
    n_tp = len(tokens) // 2
    rows, wide = tokens[0].shape
    half = sum(both.shape[0] for both in boths) // 2
    work = count * 2 * rows
    vmem = pl.BlockSpec(memory_space=pltpu.VMEM)
    return pl.pallas_call(
        functools.partial(hidden_kernel, depth, n_tp, first, len(boths)),
        grid=(count, 2),
        in_specs=[pl.BlockSpec(memory_space=pltpu.SMEM), *[vmem] * (len(boths) + len(tokens))],
        out_specs=pl.BlockSpec((1, 1, rows, half), lambda q, c: (q, c, 0, 0)),
        out_shape=jax.ShapeDtypeStruct((count, 2, rows, half), BF16),
        scratch_shapes=[pltpu.VMEM((rows, wide), BF16)],
        compiler_params=params("arbitrary", "arbitrary"),
        cost_estimate=pl.CostEstimate(
            flops=2 * work * depth * 2 * half, bytes_accessed=work * wide * 2, transcendentals=work * half
        ),
        name="hidden",
    )(place, *boths, *tokens)


def down_kernel(place_ref, down_ref, *refs):
    pieces, (keep_ref, send_ref) = refs[:-2], refs[-2:]
    experts = down_ref.shape[0]
    total = None
    for shift in range(experts):
        parts = [ref[0].reshape(-1, ref.shape[3]) for ref in pieces[shift::experts]]
        left = jnp.concatenate(parts, axis=1) if len(parts) > 1 else parts[0]
        source = lax.rem(place_ref[0] + experts - shift, experts)
        term = jnp.dot(left, down_ref[source], preferred_element_type=F32)
        total = term if total is None else total + term
    rows = total.shape[0] // 2
    mine = place_ref[1] == 0
    even, odd = total[:rows], total[rows:]
    keep = jnp.where(mine, even, odd)
    send = jnp.where(mine, odd, even).astype(BF16)
    keep_ref[...] = keep.reshape(keep_ref.shape)
    send_ref[...] = send.reshape(send_ref.shape)


def down_of(place, down, pieces, n_z):
    features = down.shape[2]
    count, _, rows, _ = pieces[0].shape
    out = pl.BlockSpec((n_z, 1, rows // n_z, features), lambda q: (0, q, 0, 0))
    shape = (n_z, count, rows // n_z, features)
    return pl.pallas_call(
        down_kernel,
        grid=(count,),
        in_specs=[
            pl.BlockSpec(memory_space=pltpu.SMEM),
            pl.BlockSpec(down.shape, lambda q: (0, 0, 0)),
            *[pl.BlockSpec((1, 2, rows, piece.shape[3]), lambda q: (q, 0, 0, 0)) for piece in pieces],
        ],
        out_specs=[out, out],
        out_shape=[jax.ShapeDtypeStruct(shape, F32), jax.ShapeDtypeStruct(shape, BF16)],
        compiler_params=params("arbitrary"),
        cost_estimate=pl.CostEstimate(
            flops=4 * count * rows * down.size, bytes_accessed=count * rows * 2 * (features * 3 + 2048), transcendentals=0
        ),
        name="down",
    )(place, down, *pieces)


def held_kernel(in_ref, out_ref):
    out_ref[...] = in_ref[...]


def held(array):
    vmem = pl.BlockSpec(memory_space=pltpu.VMEM)
    return pl.pallas_call(
        held_kernel,
        in_specs=[vmem],
        out_specs=vmem,
        out_shape=jax.ShapeDtypeStruct(array.shape, array.dtype),
        compiler_params=params(),
        cost_estimate=pl.CostEstimate(flops=array.size * 500, bytes_accessed=array.size * 4, transcendentals=0),
        name="held",
    )(array)


def around(array, axis):
    n = lax.axis_size(axis)
    got = {0: array}
    for shift in [1, n - 1, *range(2, n - 1)]:
        got[shift] = lax.ppermute(array, axis, [(i, (i + shift) % n) for i in range(n)])
    return [got[shift] for shift in range(n)]


def dealt(pieces, axis):
    n = lax.axis_size(axis)
    got = {0: pieces[0]}
    for shift in [1, n - 1, *range(2, n - 1)]:
        got[shift] = lax.ppermute(pieces[shift], axis, [(i, (i + shift) % n) for i in range(n)])
    return [got[shift] for shift in range(n)]


def body(chunks, tokens, routes, route_logits, gain, w_gate, w_up, w_down):
    n_fs, n_tp = lax.axis_size("fs"), lax.axis_size("tp")
    _, hidden_rows, features = w_down.shape
    count, depth = tokens.shape
    me = lax.axis_index("fs")
    expert = lax.axis_index("tp").astype(jnp.int32)
    place = jnp.stack([expert, (me % 2).astype(jnp.int32)])
    parts = ((0, LANES), (LANES, hidden_rows - LANES))
    swap = [(i, i + 1 - 2 * (i % 2)) for i in range(n_fs)]
    columns = [list(range(c, n_fs, 2)) for c in range(2)]
    n_z = n_fs // 2

    some = count // n_tp
    tokens, routes, route_logits = (
        lax.dynamic_slice_in_dim(a, expert * some, some) for a in (tokens, routes, route_logits)
    )
    values = tokens.astype(F32)
    mean_square = jnp.mean(values * values, axis=-1, keepdims=True)
    normed = (values * lax.rsqrt(mean_square + 1e-06)).astype(BF16)
    first = jax.nn.sigmoid(route_logits[:, 0:1] - route_logits[:, 1:2])
    second = jax.nn.sigmoid(route_logits[:, 1:2] - route_logits[:, 0:1])
    names = lax.broadcasted_iota(jnp.int32, (some, LANES), 1)
    share = first * (routes[:, 0:1] == names).astype(F32)
    share = (share + second * (routes[:, 1:2] == names).astype(F32)).astype(BF16)
    rows = jnp.concatenate([normed, share], axis=1)
    rows, place = lax.optimization_barrier((rows, place))
    quarter = lax.all_gather(rows, "fs", axis=0, axis_index_groups=columns, tiled=True)
    first_part, late_parts = pack(place, gain, w_gate, w_up, parts, hidden_rows)
    first_part = first_part.reshape(n_tp, -1, first_part.shape[3])
    across = lax.all_to_all(first_part, "tp", 0, 0, tiled=True).reshape(n_fs, -1, first_part.shape[2])
    received = lax.all_to_all(across, "fs", 0, 0, tiled=True)
    late_across = join(place, dealt(late_parts, "tp"), 0)
    late_across, received = lax.optimization_barrier((late_across, received))
    late_received = lax.all_to_all(late_across, "fs", 0, 0, tiled=True)

    quarter = held(quarter)
    quarters = around(quarter, "tp")
    all_tokens = []
    for piece in quarters:
        all_tokens += [piece, lax.ppermute(piece, "fs", swap)]

    down_padded, down_pieces = cast_down(place, w_down, len(parts) * LANES)
    down_pieces = dealt(down_pieces, "tp")
    down_served = join(place, down_pieces, 1)[None]

    per = n_tp // chunks
    gate_a, up_a, both_a = unpack(received, LANES)
    hidden = hidden_of(place, all_tokens, (both_a,), depth, 0, per)
    gathered = [around(hidden, "tp")]
    gate_b, up_b, both_b = unpack(late_received, LANES)
    gates, ups = (gate_a, gate_b), (up_a, up_b)
    hidden = hidden_of(place, all_tokens, (both_b,), depth, 0, per)
    gathered[0] = gathered[0] + around(hidden, "tp")
    for q in range(1, chunks):
        hidden = hidden_of(place, all_tokens, (both_a, both_b), depth, q * per, per)
        gathered.append(around(hidden, "tp"))
    out = []
    for q in range(chunks):
        keep, send = down_of(place, down_padded, gathered[q], n_z)
        summed = (keep + lax.ppermute(send, "fs", swap).astype(F32)).astype(BF16)
        summed = summed.reshape(n_z, per * some, features)
        spread = lax.all_to_all(summed, "fs", 0, 0, axis_index_groups=columns, tiled=True)
        out.append(jnp.sum(spread.astype(F32), axis=0).astype(BF16))
    mixed = jnp.concatenate(out, axis=0)
    gate_served = jnp.concatenate(gates, axis=0).T[None]
    up_served = jnp.concatenate(ups, axis=0).T[None]
    return gate_served, up_served, down_served, mixed


def layer(chunks, *args):
    return body(chunks, *args)


def solution(mesh):
    return jax.shard_map(
        functools.partial(layer, 2),
        mesh=mesh,
        in_specs=(
            P(("grp", "fs"), None),
            P(("grp", "fs"), None),
            P(("grp", "fs"), None),
            P("fs"),
            P(None, "fs", "tp"),
            P(None, "fs", "tp"),
            P(None, "fs", "tp"),
        ),
        out_specs=(
            P(("grp", "tp"), None, "fs"),
            P(("grp", "tp"), None, "fs"),
            P(("grp", "tp"), "fs", None),
            P(("grp", "fs"), "tp"),
        ),
        check_vma=False,
    )
```

```python
import functools

import jax
import jax.numpy as jnp
from jax import lax
from jax.experimental import pallas as pl
from jax.experimental.pallas import tpu as pltpu
from jax.sharding import PartitionSpec as P

BF16, F32 = jnp.bfloat16, jnp.float32
LANES = 128
VMEM = 56 * 1024 * 1024


def params(*semantics):
    return pltpu.CompilerParams(dimension_semantics=semantics, vmem_limit_bytes=VMEM)


def pack_kernel(parts, width, place_ref, scale_ref, gate_ref, up_ref, first_ref, *late_refs):
    del place_ref
    both = jnp.concatenate([gate_ref[0], up_ref[0]], axis=0)
    columns = (both.T * scale_ref[...]).astype(BF16)
    blocks = columns.shape[0] // width
    for k in range(blocks):
        low, size = parts[0]
        first_ref[0, k] = columns[k * width + low : k * width + low + size]
    for shift, late_ref in enumerate(late_refs):

        @pl.when(pl.program_id(0) == shift)
        def _():
            low, size = parts[1]
            for k in range(blocks):
                late_ref[k] = columns[k * width + low : k * width + low + size]


def pack(place, gain, w_gate, w_up, parts, width):
    experts, rows, columns = w_gate.shape
    scale = jnp.concatenate([gain, gain])[None, :]
    blocks = columns // width
    chosen = lambda s, place_ref: (lax.rem(s + place_ref[0], experts), 0, 0)
    out = pl.pallas_call(
        functools.partial(pack_kernel, parts, width),
        grid_spec=pltpu.PrefetchScalarGridSpec(
            num_scalar_prefetch=1,
            grid=(experts,),
            in_specs=[
                pl.BlockSpec((1, 2 * rows), lambda s, place_ref: (0, 0)),
                pl.BlockSpec((1, rows, columns), chosen),
                pl.BlockSpec((1, rows, columns), chosen),
            ],
            out_specs=[
                pl.BlockSpec(
                    (1, blocks, parts[0][1], 2 * rows),
                    lambda s, place_ref: (lax.rem(s + place_ref[0], experts), 0, 0, 0),
                ),
                *[pl.BlockSpec((blocks, parts[1][1], 2 * rows), lambda s, place_ref: (0, 0, 0))] * experts,
            ],
        ),
        out_shape=[
            jax.ShapeDtypeStruct((experts, blocks, parts[0][1], 2 * rows), BF16),
            *[jax.ShapeDtypeStruct((blocks, parts[1][1], 2 * rows), BF16)] * experts,
        ],
        compiler_params=params("arbitrary"),
        cost_estimate=pl.CostEstimate(
            flops=experts * rows * columns * 1000, bytes_accessed=experts * rows * columns * 12, transcendentals=0
        ),
        name="pack",
    )(place, scale, w_gate, w_up)
    return out[0], out[1:]


def cast_kernel(place_ref, down_ref, padded_ref, *piece_refs):
    del place_ref
    rows = down_ref.shape[1]
    cast = down_ref[0].astype(BF16)
    padded_ref[0, :rows] = cast
    padded_ref[0, rows:] = jnp.zeros((padded_ref.shape[1] - rows, cast.shape[1]), BF16)
    for shift, piece_ref in enumerate(piece_refs):

        @pl.when(pl.program_id(0) == shift)
        def _():
            piece_ref[...] = cast


def cast_down(place, w_down, padded):
    experts, rows, features = w_down.shape
    out = pl.pallas_call(
        cast_kernel,
        grid_spec=pltpu.PrefetchScalarGridSpec(
            num_scalar_prefetch=1,
            grid=(experts,),
            in_specs=[pl.BlockSpec((1, rows, features), lambda s, p: (lax.rem(s + p[0], experts), 0, 0))],
            out_specs=[
                pl.BlockSpec((1, padded, features), lambda s, p: (lax.rem(s + p[0], experts), 0, 0)),
                *[pl.BlockSpec((rows, features), lambda s, p: (0, 0))] * experts,
            ],
        ),
        out_shape=[
            jax.ShapeDtypeStruct((experts, padded, features), BF16),
            *[jax.ShapeDtypeStruct((rows, features), BF16)] * experts,
        ],
        compiler_params=params("arbitrary"),
        cost_estimate=pl.CostEstimate(flops=w_down.size * 500, bytes_accessed=w_down.size * 8, transcendentals=0),
        name="cast_down",
    )(place, w_down)
    return out[0], out[1:]


def join_kernel(place_ref, *refs):
    del place_ref
    out_ref = refs[-1]
    for shift, ref in enumerate(refs[:-1]):

        @pl.when(pl.program_id(0) == shift)
        def _():
            out_ref[...] = ref[...]


def join(place, pieces, dim):
    n, dims = len(pieces), pieces[0].shape
    spot = lambda s, p: tuple(lax.rem(p[0] + n - s, n) if d == dim else 0 for d in range(len(dims)))
    whole = tuple(size * n if d == dim else size for d, size in enumerate(dims))
    return pl.pallas_call(
        join_kernel,
        grid_spec=pltpu.PrefetchScalarGridSpec(
            num_scalar_prefetch=1,
            grid=(n,),
            in_specs=[pl.BlockSpec(dims, lambda s, p: (0,) * len(dims))] * n,
            out_specs=pl.BlockSpec(dims, spot),
        ),
        out_shape=jax.ShapeDtypeStruct(whole, BF16),
        compiler_params=params("arbitrary"),
        cost_estimate=pl.CostEstimate(flops=pieces[0].size * n * 500, bytes_accessed=pieces[0].size * n * 4, transcendentals=0),
        name="join",
    )(place, *pieces)


def unpack_kernel(size, recv_ref, gate_ref, up_ref, both_ref):
    half = recv_ref.shape[2] // 2
    pad = both_ref.shape[0] // 2 - size
    if pad:
        zeros = jnp.zeros((pad, both_ref.shape[1]), BF16)
        both_ref[size : size + pad] = zeros
        both_ref[size + pad + size :] = zeros
    for k in range(recv_ref.shape[0] // 2):
        one, two = recv_ref[2 * k], recv_ref[2 * k + 1]
        at = slice(k * 2 * half, (k + 1) * 2 * half)
        gate = jnp.concatenate([one[:, :half], two[:, :half]], axis=1)
        up = jnp.concatenate([one[:, half:], two[:, half:]], axis=1)
        gate_ref[:, at] = gate
        up_ref[:, at] = up
        both_ref[0:size, at] = gate
        both_ref[size + pad : size + pad + size, at] = up


def unpack(recv, padded):
    count, size, lanes = recv.shape
    width = count * lanes // 2
    return pl.pallas_call(
        functools.partial(unpack_kernel, size),
        in_specs=[pl.BlockSpec(memory_space=pltpu.VMEM)],
        out_specs=[pl.BlockSpec(memory_space=pltpu.VMEM)] * 3,
        out_shape=[
            jax.ShapeDtypeStruct((size, width), BF16),
            jax.ShapeDtypeStruct((size, width), BF16),
            jax.ShapeDtypeStruct((2 * padded, width), BF16),
        ],
        compiler_params=params(),
        cost_estimate=pl.CostEstimate(flops=count * size * lanes * 40, bytes_accessed=count * size * lanes * 6, transcendentals=0),
        name="unpack",
    )(recv)


def hidden_kernel(depth, n_tp, first, n_parts, place_ref, *refs):
    both_refs, token_refs, (out_ref, held_ref, sems) = refs[:n_parts], refs[n_parts:-3], refs[-3:]
    blocks = held_ref.shape[0]
    for i in range(blocks):
        shift = lax.rem(place_ref[0] + n_tp - (first + i // 2), n_tp)
        other = jnp.where(place_ref[1] == i % 2, 0, 1)
        for k, token_ref in enumerate(token_refs):

            @pl.when(2 * shift + other == k)
            def _():
                pltpu.make_async_copy(token_ref, held_ref.at[i], sems.at[i]).start()

    def step(i, carry):
        pltpu.make_async_copy(token_refs[0], held_ref.at[i], sems.at[i]).wait()
        tokens = held_ref[i, :, :depth]
        shares = held_ref[i, :, depth:].astype(F32)
        lane = lax.broadcasted_iota(jnp.int32, shares.shape, 1)
        share = jnp.sum(jnp.where(lane == place_ref[0], shares, 0.0), axis=1, keepdims=True)
        at = 0
        for both_ref in both_refs:
            acts = lax.dot_general(
                tokens, both_ref[...], (((1,), (1,)), ((), ())), preferred_element_type=F32
            )
            half = acts.shape[1] // 2
            gate, up = acts[:, :half], acts[:, half:]
            hidden = gate / (1.0 + jnp.exp(-gate)) * up * share
            out_ref[i, :, at : at + half] = hidden.astype(BF16)
            at += half
        return carry

    lax.fori_loop(0, blocks, step, 0)


def hidden_of(place, tokens, boths, depth, first, count):
    n_tp = len(tokens) // 2
    rows, wide = tokens[0].shape
    half = sum(both.shape[0] for both in boths) // 2
    blocks = 2 * count
    vmem = pl.BlockSpec(memory_space=pltpu.VMEM)
    out = pl.pallas_call(
        functools.partial(hidden_kernel, depth, n_tp, first, len(boths)),
        in_specs=[
            pl.BlockSpec(memory_space=pltpu.SMEM),
            *[vmem] * len(boths),
            *[pl.BlockSpec(memory_space=pl.ANY)] * len(tokens),
        ],
        out_specs=vmem,
        out_shape=jax.ShapeDtypeStruct((blocks, rows, half), BF16),
        scratch_shapes=[pltpu.VMEM((blocks, rows, wide), BF16), pltpu.SemaphoreType.DMA((blocks,))],
        compiler_params=params(),
        cost_estimate=pl.CostEstimate(
            flops=4 * blocks * rows * depth * half, bytes_accessed=blocks * rows * wide * 2, transcendentals=blocks * rows * half
        ),
        name="hidden",
    )(place, *boths, *tokens)
    return out.reshape(count, 2, rows, half)


def down_kernel(place_ref, down_ref, *refs):
    pieces, (keep_ref, send_ref) = refs[:-2], refs[-2:]
    experts = down_ref.shape[0]
    total = None
    for shift in range(experts):
        parts = [ref[0].reshape(-1, ref.shape[3]) for ref in pieces[shift::experts]]
        left = jnp.concatenate(parts, axis=1) if len(parts) > 1 else parts[0]
        source = lax.rem(place_ref[0] + experts - shift, experts)
        term = jnp.dot(left, down_ref[source], preferred_element_type=F32)
        total = term if total is None else total + term
    rows = total.shape[0] // 2
    mine = place_ref[1] == 0
    even, odd = total[:rows], total[rows:]
    keep = jnp.where(mine, even, odd)
    send = jnp.where(mine, odd, even).astype(BF16)
    keep_ref[...] = keep.astype(BF16).reshape(keep_ref.shape)
    send_ref[...] = send.reshape(send_ref.shape)


def down_of(place, down, pieces, n_z):
    features = down.shape[2]
    count, _, rows, _ = pieces[0].shape
    out = pl.BlockSpec((n_z, 1, rows // n_z, features), lambda q: (0, q, 0, 0))
    shape = (n_z, count, rows // n_z, features)
    return pl.pallas_call(
        down_kernel,
        grid=(count,),
        in_specs=[
            pl.BlockSpec(memory_space=pltpu.SMEM),
            pl.BlockSpec(down.shape, lambda q: (0, 0, 0)),
            *[pl.BlockSpec((1, 2, rows, piece.shape[3]), lambda q: (q, 0, 0, 0)) for piece in pieces],
        ],
        out_specs=[out, out],
        out_shape=[jax.ShapeDtypeStruct(shape, BF16)] * 2,
        compiler_params=params("arbitrary"),
        cost_estimate=pl.CostEstimate(
            flops=4 * count * rows * down.size, bytes_accessed=count * rows * 2 * (features * 3 + 2048), transcendentals=0
        ),
        name="down",
    )(place, down, *pieces)


def held_kernel(in_ref, out_ref):
    out_ref[...] = in_ref[...]


def held(array):
    vmem = pl.BlockSpec(memory_space=pltpu.VMEM)
    return pl.pallas_call(
        held_kernel,
        in_specs=[vmem],
        out_specs=vmem,
        out_shape=jax.ShapeDtypeStruct(array.shape, array.dtype),
        compiler_params=params(),
        cost_estimate=pl.CostEstimate(flops=array.size * 500, bytes_accessed=array.size * 4, transcendentals=0),
        name="held",
    )(array)


def around(array, axis):
    n = lax.axis_size(axis)
    got = {0: array}
    for shift in [1, n - 1, *range(2, n - 1)]:
        got[shift] = lax.ppermute(array, axis, [(i, (i + shift) % n) for i in range(n)])
    return [got[shift] for shift in range(n)]


def dealt(pieces, axis):
    n = lax.axis_size(axis)
    got = {0: pieces[0]}
    for shift in [1, n - 1, *range(2, n - 1)]:
        got[shift] = lax.ppermute(pieces[shift], axis, [(i, (i + shift) % n) for i in range(n)])
    return [got[shift] for shift in range(n)]


def body(chunks, tokens, routes, route_logits, gain, w_gate, w_up, w_down):
    n_fs, n_tp = lax.axis_size("fs"), lax.axis_size("tp")
    _, hidden_rows, features = w_down.shape
    count, depth = tokens.shape
    me = lax.axis_index("fs")
    expert = lax.axis_index("tp").astype(jnp.int32)
    place = jnp.stack([expert, (me % 2).astype(jnp.int32)])
    parts = ((0, LANES), (LANES, hidden_rows - LANES))
    swap = [(i, i + 1 - 2 * (i % 2)) for i in range(n_fs)]
    columns = [list(range(c, n_fs, 2)) for c in range(2)]
    n_z = n_fs // 2

    some = count // n_tp
    tokens, routes, route_logits = (
        lax.dynamic_slice_in_dim(a, expert * some, some) for a in (tokens, routes, route_logits)
    )
    values = tokens.astype(F32)
    mean_square = jnp.mean(values * values, axis=-1, keepdims=True)
    normed = (values * lax.rsqrt(mean_square + 1e-06)).astype(BF16)
    first = jax.nn.sigmoid(route_logits[:, 0:1] - route_logits[:, 1:2])
    second = jax.nn.sigmoid(route_logits[:, 1:2] - route_logits[:, 0:1])
    names = lax.broadcasted_iota(jnp.int32, (some, LANES), 1)
    share = first * (routes[:, 0:1] == names).astype(F32)
    share = (share + second * (routes[:, 1:2] == names).astype(F32)).astype(BF16)
    rows = jnp.concatenate([normed, share], axis=1)
    rows, place = lax.optimization_barrier((rows, place))
    quarter = lax.all_gather(rows, "fs", axis=0, axis_index_groups=columns, tiled=True)
    first_part, late_parts = pack(place, gain, w_gate, w_up, parts, hidden_rows)
    first_part = first_part.reshape(n_tp, -1, first_part.shape[3])
    across = lax.all_to_all(first_part, "tp", 0, 0, tiled=True).reshape(n_fs, -1, first_part.shape[2])
    received = lax.all_to_all(across, "fs", 0, 0, tiled=True)
    late_across = join(place, dealt(late_parts, "tp"), 0)
    late_across, received = lax.optimization_barrier((late_across, received))
    late_received = lax.all_to_all(late_across, "fs", 0, 0, tiled=True)

    quarter = held(quarter)
    quarters = around(quarter, "tp")
    all_tokens = []
    for piece in quarters:
        all_tokens += [piece, lax.ppermute(piece, "fs", swap)]

    down_padded, down_pieces = cast_down(place, w_down, len(parts) * LANES)
    down_pieces = dealt(down_pieces, "tp")
    down_served = join(place, down_pieces, 1)[None]

    per = n_tp // chunks
    gate_a, up_a, both_a = unpack(received, LANES)
    hidden = hidden_of(place, all_tokens, (both_a,), depth, 0, per)
    gathered = [around(hidden, "tp")]
    gate_b, up_b, both_b = unpack(late_received, LANES)
    gates, ups = (gate_a, gate_b), (up_a, up_b)
    hidden = hidden_of(place, all_tokens, (both_b,), depth, 0, per)
    gathered[0] = gathered[0] + around(hidden, "tp")
    for q in range(1, chunks):
        hidden = hidden_of(place, all_tokens, (both_a, both_b), depth, q * per, per)
        gathered.append(around(hidden, "tp"))
    out = []
    for q in range(chunks):
        keep, send = down_of(place, down_padded, gathered[q], n_z)
        summed = (keep.astype(F32) + lax.ppermute(send, "fs", swap).astype(F32)).astype(BF16)
        summed = summed.reshape(n_z, per * some, features)
        spread = lax.all_to_all(summed, "fs", 0, 0, axis_index_groups=columns, tiled=True)
        out.append(jnp.sum(spread.astype(F32), axis=0).astype(BF16))
    mixed = jnp.concatenate(out, axis=0)
    gate_served = jnp.concatenate(gates, axis=0).T[None]
    up_served = jnp.concatenate(ups, axis=0).T[None]
    return gate_served, up_served, down_served, mixed


def layer(chunks, *args):
    return body(chunks, *args)


def solution(mesh):
    return jax.shard_map(
        functools.partial(layer, 2),
        mesh=mesh,
        in_specs=(
            P(("grp", "fs"), None),
            P(("grp", "fs"), None),
            P(("grp", "fs"), None),
            P("fs"),
            P(None, "fs", "tp"),
            P(None, "fs", "tp"),
            P(None, "fs", "tp"),
        ),
        out_specs=(
            P(("grp", "tp"), None, "fs"),
            P(("grp", "tp"), None, "fs"),
            P(("grp", "tp"), "fs", None),
            P(("grp", "fs"), "tp"),
        ),
        check_vma=False,
    )
```

```python
import functools

import jax
import jax.numpy as jnp
from jax import lax
from jax.experimental import pallas as pl
from jax.experimental.pallas import tpu as pltpu
from jax.sharding import PartitionSpec as P

BF16, F32 = jnp.bfloat16, jnp.float32
LANES = 128
VMEM = 56 * 1024 * 1024


def params(*semantics):
    return pltpu.CompilerParams(dimension_semantics=semantics, vmem_limit_bytes=VMEM)


def rows_kernel(place_ref, tokens_ref, routes_ref, logits_ref, out_ref):
    values = tokens_ref[...].astype(F32)
    rows, depth = values.shape
    mean_square = jnp.mean(values * values, axis=-1, keepdims=True)
    out_ref[:, :depth] = (values * lax.rsqrt(mean_square + 1e-06)).astype(BF16)
    dims = (rows, routes_ref.shape[1])
    spot = place_ref[0] * rows + lax.broadcasted_iota(jnp.int32, dims, 0)
    mine = lax.broadcasted_iota(jnp.int32, dims, 1) == spot

    def column(row):
        return jnp.sum(jnp.where(mine, row, 0.0), axis=1, keepdims=True)

    names = lax.broadcasted_iota(jnp.int32, (rows, LANES), 1).astype(F32)
    logits = [column(logits_ref[k : k + 1]) for k in range(2)]
    share = 0.0
    for k in range(2):
        weight = 1.0 / (1.0 + jnp.exp(logits[1 - k] - logits[k]))
        named = column(routes_ref[k : k + 1].astype(F32)) == names
        share = share + jnp.where(named, weight, 0.0)
    out_ref[:, depth:] = share.astype(BF16)


def rows_of(place, tokens, routes, route_logits, some):
    count, depth = tokens.shape
    return pl.pallas_call(
        rows_kernel,
        grid_spec=pltpu.PrefetchScalarGridSpec(
            num_scalar_prefetch=1,
            grid=(1,),
            in_specs=[
                pl.BlockSpec((some, depth), lambda i, p: (p[0], 0)),
                pl.BlockSpec((2, count), lambda i, p: (0, 0)),
                pl.BlockSpec((2, count), lambda i, p: (0, 0)),
            ],
            out_specs=pl.BlockSpec((some, depth + LANES), lambda i, p: (0, 0)),
        ),
        out_shape=jax.ShapeDtypeStruct((some, depth + LANES), BF16),
        compiler_params=params("arbitrary"),
        cost_estimate=pl.CostEstimate(flops=some * depth * 1000, bytes_accessed=some * depth * 4, transcendentals=some * 4),
        name="rows",
    )(place, tokens, routes.T, route_logits.T)


def pack_kernel(parts, width, place_ref, scale_ref, gate_ref, up_ref, first_ref, *late_refs):
    del place_ref
    both = jnp.concatenate([gate_ref[0], up_ref[0]], axis=0)
    columns = (both.T * jnp.concatenate([scale_ref[...]] * 2, axis=1)).astype(BF16)
    blocks = columns.shape[0] // width
    for k in range(blocks):
        low, size = parts[0]
        first_ref[0, k] = columns[k * width + low : k * width + low + size]
    for shift, late_ref in enumerate(late_refs):

        @pl.when(pl.program_id(0) == shift)
        def _():
            low, size = parts[1]
            for k in range(blocks):
                late_ref[k] = columns[k * width + low : k * width + low + size]


def pack(place, gain, w_gate, w_up, parts, width):
    experts, rows, columns = w_gate.shape
    scale = gain[None, :]
    blocks = columns // width
    chosen = lambda s, place_ref: (lax.rem(s + place_ref[0], experts), 0, 0)
    out = pl.pallas_call(
        functools.partial(pack_kernel, parts, width),
        grid_spec=pltpu.PrefetchScalarGridSpec(
            num_scalar_prefetch=1,
            grid=(experts,),
            in_specs=[
                pl.BlockSpec((1, rows), lambda s, place_ref: (0, 0)),
                pl.BlockSpec((1, rows, columns), chosen),
                pl.BlockSpec((1, rows, columns), chosen),
            ],
            out_specs=[
                pl.BlockSpec(
                    (1, blocks, parts[0][1], 2 * rows),
                    lambda s, place_ref: (lax.rem(s + place_ref[0], experts), 0, 0, 0),
                ),
                *[pl.BlockSpec((blocks, parts[1][1], 2 * rows), lambda s, place_ref: (0, 0, 0))] * experts,
            ],
        ),
        out_shape=[
            jax.ShapeDtypeStruct((experts, blocks, parts[0][1], 2 * rows), BF16),
            *[jax.ShapeDtypeStruct((blocks, parts[1][1], 2 * rows), BF16)] * experts,
        ],
        compiler_params=params("arbitrary"),
        cost_estimate=pl.CostEstimate(
            flops=experts * rows * columns * 1000, bytes_accessed=experts * rows * columns * 12, transcendentals=0
        ),
        name="pack",
    )(place, scale, w_gate, w_up)
    return out[0], out[1:]


def cast_kernel(place_ref, down_ref, padded_ref, *piece_refs):
    del place_ref
    rows = down_ref.shape[1]
    cast = down_ref[0].astype(BF16)
    padded_ref[0, :rows] = cast
    padded_ref[0, rows:] = jnp.zeros((padded_ref.shape[1] - rows, cast.shape[1]), BF16)
    for shift, piece_ref in enumerate(piece_refs):

        @pl.when(pl.program_id(0) == shift)
        def _():
            piece_ref[...] = cast


def cast_down(place, w_down, padded):
    experts, rows, features = w_down.shape
    out = pl.pallas_call(
        cast_kernel,
        grid_spec=pltpu.PrefetchScalarGridSpec(
            num_scalar_prefetch=1,
            grid=(experts,),
            in_specs=[pl.BlockSpec((1, rows, features), lambda s, p: (lax.rem(s + p[0], experts), 0, 0))],
            out_specs=[
                pl.BlockSpec((1, padded, features), lambda s, p: (lax.rem(s + p[0], experts), 0, 0)),
                *[pl.BlockSpec((rows, features), lambda s, p: (0, 0))] * experts,
            ],
        ),
        out_shape=[
            jax.ShapeDtypeStruct((experts, padded, features), BF16),
            *[jax.ShapeDtypeStruct((rows, features), BF16)] * experts,
        ],
        compiler_params=params("arbitrary"),
        cost_estimate=pl.CostEstimate(flops=w_down.size * 500, bytes_accessed=w_down.size * 8, transcendentals=0),
        name="cast_down",
    )(place, w_down)
    return out[0], out[1:]


def join_kernel(place_ref, *refs):
    del place_ref
    out_ref = refs[-1]
    for shift, ref in enumerate(refs[:-1]):

        @pl.when(pl.program_id(0) == shift)
        def _():
            out_ref[...] = ref[...]


def join(place, pieces, dim):
    n, dims = len(pieces), pieces[0].shape
    spot = lambda s, p: tuple(lax.rem(p[0] + n - s, n) if d == dim else 0 for d in range(len(dims)))
    whole = tuple(size * n if d == dim else size for d, size in enumerate(dims))
    return pl.pallas_call(
        join_kernel,
        grid_spec=pltpu.PrefetchScalarGridSpec(
            num_scalar_prefetch=1,
            grid=(n,),
            in_specs=[pl.BlockSpec(dims, lambda s, p: (0,) * len(dims))] * n,
            out_specs=pl.BlockSpec(dims, spot),
        ),
        out_shape=jax.ShapeDtypeStruct(whole, BF16),
        compiler_params=params("arbitrary"),
        cost_estimate=pl.CostEstimate(flops=pieces[0].size * n * 500, bytes_accessed=pieces[0].size * n * 4, transcendentals=0),
        name="join",
    )(place, *pieces)


def unpack_kernel(size, recv_ref, gate_ref, up_ref, both_ref):
    half = recv_ref.shape[2] // 2
    pad = both_ref.shape[0] // 2 - size
    if pad:
        zeros = jnp.zeros((pad, both_ref.shape[1]), BF16)
        both_ref[size : size + pad] = zeros
        both_ref[size + pad + size :] = zeros
    for k in range(recv_ref.shape[0] // 2):
        one, two = recv_ref[2 * k], recv_ref[2 * k + 1]
        at = slice(k * 2 * half, (k + 1) * 2 * half)
        gate = jnp.concatenate([one[:, :half], two[:, :half]], axis=1)
        up = jnp.concatenate([one[:, half:], two[:, half:]], axis=1)
        gate_ref[:, at] = gate
        up_ref[:, at] = up
        both_ref[0:size, at] = gate
        both_ref[size + pad : size + pad + size, at] = up


def unpack(recv, padded):
    count, size, lanes = recv.shape
    width = count * lanes // 2
    return pl.pallas_call(
        functools.partial(unpack_kernel, size),
        in_specs=[pl.BlockSpec(memory_space=pltpu.VMEM)],
        out_specs=[pl.BlockSpec(memory_space=pltpu.VMEM)] * 3,
        out_shape=[
            jax.ShapeDtypeStruct((size, width), BF16),
            jax.ShapeDtypeStruct((size, width), BF16),
            jax.ShapeDtypeStruct((2 * padded, width), BF16),
        ],
        compiler_params=params(),
        cost_estimate=pl.CostEstimate(flops=count * size * lanes * 40, bytes_accessed=count * size * lanes * 6, transcendentals=0),
        name="unpack",
    )(recv)


def hidden_kernel(depth, n_tp, first, n_parts, place_ref, *refs):
    both_refs, token_refs, (out_ref, held_ref, sems) = refs[:n_parts], refs[n_parts:-3], refs[-3:]
    blocks = held_ref.shape[0]
    for i in range(blocks):
        shift = lax.rem(place_ref[0] + n_tp - (first + i // 2), n_tp)
        other = jnp.where(place_ref[1] == i % 2, 0, 1)
        for k, token_ref in enumerate(token_refs):

            @pl.when(2 * shift + other == k)
            def _():
                pltpu.make_async_copy(token_ref, held_ref.at[i], sems.at[i]).start()

    def step(i, carry):
        pltpu.make_async_copy(token_refs[0], held_ref.at[i], sems.at[i]).wait()
        tokens = held_ref[i, :, :depth]
        shares = held_ref[i, :, depth:].astype(F32)
        lane = lax.broadcasted_iota(jnp.int32, shares.shape, 1)
        share = jnp.sum(jnp.where(lane == place_ref[0], shares, 0.0), axis=1, keepdims=True)
        at = 0
        for both_ref in both_refs:
            acts = lax.dot_general(
                tokens, both_ref[...], (((1,), (1,)), ((), ())), preferred_element_type=F32
            )
            half = acts.shape[1] // 2
            gate, up = acts[:, :half], acts[:, half:]
            hidden = gate / (1.0 + jnp.exp(-gate)) * up * share
            out_ref[i, :, at : at + half] = hidden.astype(BF16)
            at += half
        return carry

    lax.fori_loop(0, blocks, step, 0)


def hidden_of(place, tokens, boths, depth, first, count):
    n_tp = len(tokens) // 2
    rows, wide = tokens[0].shape
    half = sum(both.shape[0] for both in boths) // 2
    blocks = 2 * count
    vmem = pl.BlockSpec(memory_space=pltpu.VMEM)
    out = pl.pallas_call(
        functools.partial(hidden_kernel, depth, n_tp, first, len(boths)),
        in_specs=[
            pl.BlockSpec(memory_space=pltpu.SMEM),
            *[vmem] * len(boths),
            *[pl.BlockSpec(memory_space=pl.ANY)] * len(tokens),
        ],
        out_specs=vmem,
        out_shape=jax.ShapeDtypeStruct((blocks, rows, half), BF16),
        scratch_shapes=[pltpu.VMEM((blocks, rows, wide), BF16), pltpu.SemaphoreType.DMA((blocks,))],
        compiler_params=params(),
        cost_estimate=pl.CostEstimate(
            flops=4 * blocks * rows * depth * half, bytes_accessed=blocks * rows * wide * 2, transcendentals=blocks * rows * half
        ),
        name="hidden",
    )(place, *boths, *tokens)
    return out.reshape(count, 2, rows, half)


def down_kernel(place_ref, down_ref, *refs):
    pieces, (keep_ref, send_ref) = refs[:-2], refs[-2:]
    experts = down_ref.shape[0]
    total = None
    for shift in range(experts):
        parts = [ref[0].reshape(-1, ref.shape[3]) for ref in pieces[shift::experts]]
        left = jnp.concatenate(parts, axis=1) if len(parts) > 1 else parts[0]
        source = lax.rem(place_ref[0] + experts - shift, experts)
        term = jnp.dot(left, down_ref[source], preferred_element_type=F32)
        total = term if total is None else total + term
    rows = total.shape[0] // 2
    mine = place_ref[1] == 0
    even, odd = total[:rows], total[rows:]
    keep = jnp.where(mine, even, odd)
    send = jnp.where(mine, odd, even).astype(BF16)
    keep_ref[...] = keep.astype(BF16).reshape(keep_ref.shape)
    send_ref[...] = send.reshape(send_ref.shape)


def down_of(place, down, pieces, n_z):
    features = down.shape[2]
    count, _, rows, _ = pieces[0].shape
    out = pl.BlockSpec((n_z, 1, rows // n_z, features), lambda q: (0, q, 0, 0))
    shape = (n_z, count, rows // n_z, features)
    return pl.pallas_call(
        down_kernel,
        grid=(count,),
        in_specs=[
            pl.BlockSpec(memory_space=pltpu.SMEM),
            pl.BlockSpec(down.shape, lambda q: (0, 0, 0)),
            *[pl.BlockSpec((1, 2, rows, piece.shape[3]), lambda q: (q, 0, 0, 0)) for piece in pieces],
        ],
        out_specs=[out, out],
        out_shape=[jax.ShapeDtypeStruct(shape, BF16)] * 2,
        compiler_params=params("arbitrary"),
        cost_estimate=pl.CostEstimate(
            flops=4 * count * rows * down.size, bytes_accessed=count * rows * 2 * (features * 3 + 2048), transcendentals=0
        ),
        name="down",
    )(place, down, *pieces)


def held_kernel(in_ref, out_ref):
    out_ref[...] = in_ref[...]


def held(array):
    vmem = pl.BlockSpec(memory_space=pltpu.VMEM)
    return pl.pallas_call(
        held_kernel,
        in_specs=[vmem],
        out_specs=vmem,
        out_shape=jax.ShapeDtypeStruct(array.shape, array.dtype),
        compiler_params=params(),
        cost_estimate=pl.CostEstimate(flops=array.size * 500, bytes_accessed=array.size * 4, transcendentals=0),
        name="held",
    )(array)


def around(array, axis):
    n = lax.axis_size(axis)
    got = {0: array}
    for shift in [1, n - 1, *range(2, n - 1)]:
        got[shift] = lax.ppermute(array, axis, [(i, (i + shift) % n) for i in range(n)])
    return [got[shift] for shift in range(n)]


def dealt(pieces, axis):
    n = lax.axis_size(axis)
    got = {0: pieces[0]}
    for shift in [1, n - 1, *range(2, n - 1)]:
        got[shift] = lax.ppermute(pieces[shift], axis, [(i, (i + shift) % n) for i in range(n)])
    return [got[shift] for shift in range(n)]


def body(chunks, tokens, routes, route_logits, gain, w_gate, w_up, w_down):
    n_fs, n_tp = lax.axis_size("fs"), lax.axis_size("tp")
    _, hidden_rows, features = w_down.shape
    count, depth = tokens.shape
    me = lax.axis_index("fs")
    expert = lax.axis_index("tp").astype(jnp.int32)
    place = jnp.stack([expert, (me % 2).astype(jnp.int32)])
    parts = ((0, LANES), (LANES, hidden_rows - LANES))
    swap = [(i, i + 1 - 2 * (i % 2)) for i in range(n_fs)]
    columns = [list(range(c, n_fs, 2)) for c in range(2)]
    n_z = n_fs // 2

    some = count // n_tp
    rows = rows_of(place, tokens, routes, route_logits, some)
    rows, place = lax.optimization_barrier((rows, place))
    quarter = lax.all_gather(rows, "fs", axis=0, axis_index_groups=columns, tiled=True)
    first_part, late_parts = pack(place, gain, w_gate, w_up, parts, hidden_rows)
    first_part = first_part.reshape(n_tp, -1, first_part.shape[3])
    across = lax.all_to_all(first_part, "tp", 0, 0, tiled=True).reshape(n_fs, -1, first_part.shape[2])
    received = lax.all_to_all(across, "fs", 0, 0, tiled=True)
    late_across = join(place, dealt(late_parts, "tp"), 0)
    late_across, received = lax.optimization_barrier((late_across, received))
    late_received = lax.all_to_all(late_across, "fs", 0, 0, tiled=True)

    quarter = held(quarter)
    quarters = around(quarter, "tp")
    all_tokens = []
    for piece in quarters:
        all_tokens += [piece, lax.ppermute(piece, "fs", swap)]

    down_padded, down_pieces = cast_down(place, w_down, len(parts) * LANES)
    down_pieces = dealt(down_pieces, "tp")
    down_served = join(place, down_pieces, 1)[None]

    per = n_tp // chunks
    gate_a, up_a, both_a = unpack(received, LANES)
    hidden = hidden_of(place, all_tokens, (both_a,), depth, 0, per)
    gathered = [around(hidden, "tp")]
    gate_b, up_b, both_b = unpack(late_received, LANES)
    gates, ups = (gate_a, gate_b), (up_a, up_b)
    hidden = hidden_of(place, all_tokens, (both_b,), depth, 0, per)
    gathered[0] = gathered[0] + around(hidden, "tp")
    for q in range(1, chunks):
        hidden = hidden_of(place, all_tokens, (both_a, both_b), depth, q * per, per)
        gathered.append(around(hidden, "tp"))
    out = []
    for q in range(chunks):
        keep, send = down_of(place, down_padded, gathered[q], n_z)
        summed = (keep.astype(F32) + lax.ppermute(send, "fs", swap).astype(F32)).astype(BF16)
        summed = summed.reshape(n_z, per * some, features)
        spread = lax.all_to_all(summed, "fs", 0, 0, axis_index_groups=columns, tiled=True)
        out.append(jnp.sum(spread.astype(F32), axis=0).astype(BF16))
    mixed = jnp.concatenate(out, axis=0)
    gate_served = jnp.concatenate(gates, axis=0).T[None]
    up_served = jnp.concatenate(ups, axis=0).T[None]
    return gate_served, up_served, down_served, mixed


def layer(chunks, *args):
    return body(chunks, *args)


def solution(mesh):
    return jax.shard_map(
        functools.partial(layer, 2),
        mesh=mesh,
        in_specs=(
            P(("grp", "fs"), None),
            P(("grp", "fs"), None),
            P(("grp", "fs"), None),
            P("fs"),
            P(None, "fs", "tp"),
            P(None, "fs", "tp"),
            P(None, "fs", "tp"),
        ),
        out_specs=(
            P(("grp", "tp"), None, "fs"),
            P(("grp", "tp"), None, "fs"),
            P(("grp", "tp"), "fs", None),
            P(("grp", "fs"), "tp"),
        ),
        check_vma=False,
    )
```
